128 devices in a mesh: fs: 16 (over z, y), tp: 8 (over x, core).
Axes of the slice: x: 4, y: 4, z: 4, core: 2. Of those that a mesh axis runs over, the one named last changes fastest.
Arguments:
- fresh_rows: bfloat16 [16384, 2048], P('fs'), may hold values from -6 to 6
- saved_rows: bfloat16 [16384, 2048], P('fs'), may hold values from -6 to 6
- upstream_grad: bfloat16 [16384, 2048], P('fs'), may hold values from -6 to 6
- proj_up: bfloat16 [2048, 8192], P('fs', 'tp'), may hold values from -0.125 to 0.125
- proj_down: bfloat16 [2048, 8192], P('fs', 'tp'), may hold values from -0.0625 to 0.0625
- accum_up: float32 [2048, 8192], P('fs', 'tp'), may hold values from -6 to 6
- accum_down: float32 [2048, 8192], P('fs', 'tp'), may hold values from -6 to 6
Outputs:
- fresh_out: bfloat16 [16384, 2048], P(('fs', 'tp'))
- saved_grad: bfloat16 [16384, 2048], P(('fs', 'tp'))
- accum_up_out: float32 [2048, 8192], P('fs', 'tp')
- accum_down_out: float32 [2048, 8192], P('fs', 'tp')
The draws below stay inside these ranges and needn't reach their ends.
All inputs are finite; a program needn't handle non-finite values.
Results may differ from the reference program's by a relative error of at most 0.014.
Values may be sent and summed in bfloat16 or wider, within the bound.
A program may use at most 128 MiB of HBM per device.

```python
import jax
import jax.numpy as jnp
from jax import lax

D = 2048
FF = 8192
TOKENS = 16384
N_TP = 8


def raised(result, stream_key, source, target, shards_of, factor):
    owner, partner = [(jnp.arange(result.shape[axis_at]) // (result.shape[axis_at] // shards_of)).reshape([-1 if axis == axis_at else 1 for axis in range(result.ndim)]) for axis_at in (source, target)]
    chosen = jax.random.permutation(stream_key, shards_of)[partner]
    strong = (owner == chosen) | (owner == (partner + shards_of // 2) % shards_of)
    return jnp.where(strong, factor * result, result)


def block_levels(key, dims, split, least, top_value):
    factor_of = 1.0
    for axis_at, parts in split:
        draws = jax.random.uniform(jax.random.fold_in(jax.random.fold_in(key, 6), axis_at), (parts,), jnp.float32, least / len(split), top_value / len(split))
        factor_of = factor_of * jnp.repeat(jnp.exp(draws), dims[axis_at] // parts).reshape((-1,) + (1,) * (len(dims) - 1 - axis_at))
    return factor_of


def gaussian(stream_key, extent, spread, reach, shards=(), held_as=jnp.bfloat16):
    level = block_levels(stream_key, extent, shards, -0.22, 0.18) if shards else 1.0
    values = jax.random.normal(stream_key, extent, jnp.float32) * spread * level
    return jnp.minimum(jnp.maximum(values, -reach), reach).astype(held_as)


def heavy_noise(rng, dims, spread, bound, cuts, heavy, held_as=jnp.bfloat16):
    drawn = spread * jax.random.normal(rng, dims, jnp.float32)
    if cuts:
        drawn = drawn * block_levels(rng, dims, cuts, -0.22, 0.18)
    return jnp.clip(raised(drawn, jax.random.fold_in(rng, 3), *heavy), -bound, bound).astype(held_as)


def setup_inputs(seed: int = 0) -> dict:
    splits = jax.random.split(jax.random.key(seed), 8)
    return {
        "fresh_rows": gaussian(splits[0], (TOKENS, D), 1.0, 6.0, ((0, 16),)),
        "saved_rows": gaussian(splits[1], (TOKENS, D), 1.0, 6.0, ((0, 16),)),
        "upstream_grad": heavy_noise(splits[2], (TOKENS, D), 1.0, 6.0, ((0, 16),), (0, 1, 16, 2.0)),
        "proj_up": gaussian(splits[3], (D, FF), D ** -0.5, 0.125, ((0, 16), (1, 8))),
        "proj_down": gaussian(splits[4], (D, FF), FF ** -0.5, 0.0625, ((0, 16), (1, 8))),
        "accum_up": gaussian(splits[5], (D, FF), 1.0, 6.0, ((0, 16), (1, 8)), jnp.float32),
        "accum_down": gaussian(splits[6], (D, FF), 1.0, 6.0, ((0, 16), (1, 8)), jnp.float32),
    }


def block_sum(left, right):
    width = FF // N_TP

    def add_block(index, running):
        first = (index * width).astype(jnp.int32)
        left_part = lax.dynamic_slice_in_dim(left, first, width, 1)
        right_part = lax.dynamic_slice_in_dim(right, first, width, 1)
        partial_sum = jnp.dot(left_part, right_part.T, preferred_element_type=jnp.float32)
        rounded = lax.optimization_barrier(partial_sum.astype(jnp.bfloat16))
        return running + rounded.astype(jnp.float32)

    empty = jnp.zeros((left.shape[0], right.shape[0]), jnp.float32)
    return lax.fori_loop(0, N_TP, add_block, empty).astype(jnp.bfloat16)


def reference(fresh_rows, saved_rows, upstream_grad, proj_up, proj_down, accum_up, accum_down):
    grad_scale = float(TOKENS) ** -0.5
    fresh_pre = jnp.dot(fresh_rows, proj_up, preferred_element_type=jnp.float32)
    fresh_active = jnp.maximum(fresh_pre, 0.0)
    fresh_hidden = (fresh_active * fresh_active).astype(jnp.bfloat16)
    fresh_out = block_sum(fresh_hidden, proj_down)
    saved_pre = jnp.dot(saved_rows, proj_up, preferred_element_type=jnp.float32)
    saved_active = jnp.maximum(saved_pre, 0.0)
    saved_hidden = (saved_active * saved_active).astype(jnp.bfloat16)
    hidden_grad = jnp.dot(upstream_grad, proj_down, preferred_element_type=jnp.float32)
    pre_grad = (2.0 * saved_active * hidden_grad).astype(jnp.bfloat16)
    saved_grad = block_sum(pre_grad, proj_up)
    up_term = jnp.dot(saved_rows.T, pre_grad, preferred_element_type=jnp.float32)
    down_term = jnp.dot(upstream_grad.T, saved_hidden, preferred_element_type=jnp.float32)
    accum_up_out = accum_up + grad_scale * up_term
    accum_down_out = accum_down + grad_scale * down_term
    return fresh_out, saved_grad, accum_up_out, accum_down_out
```

```python
import jax
import jax.numpy as jnp
from jax import lax
from jax.experimental import pallas as pl
from jax.experimental.pallas import tpu as pltpu
from jax.sharding import PartitionSpec as P

MESH = pl.DeviceIdType.MESH
BF = jnp.bfloat16
F32 = jnp.float32
COLS = (slice(0, 512), slice(512, 1024))
N_GATHER = 48
N_GRADS = 48
N_X = 20
N_MSG = N_GATHER + N_GRADS + N_X


def rows_at(start, size):
    return pl.ds(pl.multiple_of(start, size), size)


def kernel(
    fresh_hbm, saved_hbm, upstream_hbm, up_hbm, down_hbm, accum_up_hbm, accum_down_hbm,
    fresh_out, saved_grad, accum_up_out, accum_down_out,
    fresh, saved, upstream, up_w, down_w, accum_up, accum_down,
    fresh_hidden, saved_active, saved_hidden, pre_grad, grad_down, grad_up,
    land_z, land_y, land_2, land_pair, land_x,
    send_sem, recv_sem, load_sem,
):
    fs, tp = lax.axis_index("fs"), lax.axis_index("tp")
    z, y, x, core = fs // 4, fs % 4, tp // 2, tp % 2

    def nxt(p, by):
        return lax.rem(p + by, 4)

    to = {
        ("y", 1): (z * 4 + nxt(y, 1), tp),
        ("y", -1): (z * 4 + nxt(y, 3), tp),
        ("z", 1): (nxt(z, 1) * 4 + y, tp),
        ("z", -1): (nxt(z, 3) * 4 + y, tp),
        ("x", 1): (fs, nxt(x, 1) * 2 + core),
        ("x", -1): (fs, nxt(x, 3) * 2 + core),
        "pair": (fs, x * 2 + 1 - core),
    }
    place = {"y": y, "z": z, "x": x}
    used = [0]
    sent = []

    def reserve(count):
        used[0] += count
        return used[0] - count

    def message(src, dst, index, target):
        return pltpu.make_async_remote_copy(
            src_ref=src,
            dst_ref=dst,
            send_sem=send_sem.at[index],
            recv_sem=recv_sem.at[index],
            device_id=target,
            device_id_type=MESH,
        )

    def send(src, dst, index, target):
        copy = message(src, dst, index, target)
        copy.start()
        sent.append(copy)

    def arrived(dst, index, target):
        message(dst, dst, index, target).wait_recv()

    class Gather:
        def __init__(self, axis, block):
            self.plus, self.minus = to[(axis, 1)], to[(axis, -1)]
            p = place[axis]
            self.block = block
            self.here, self.after, self.across, self.before = p, nxt(p, 1), nxt(p, 2), nxt(p, 3)
            self.base = reserve(6)

        def go(self, half, index, owner, target):
            part = self.block(owner, half)
            send(part, part, self.base + index, target)

        def got(self, half, index, owner, target):
            arrived(self.block(owner, half), self.base + index, target)

        def start(self):
            self.go(0, 0, self.here, self.plus)
            self.go(1, 2, self.here, self.minus)
            self.go(1, 1, self.here, self.plus)
            self.go(0, 3, self.here, self.minus)

        def mid(self):
            self.got(0, 0, self.before, self.plus)
            self.go(0, 4, self.before, self.plus)
            self.got(1, 2, self.after, self.minus)
            self.go(1, 5, self.after, self.minus)

        def end(self):
            self.got(1, 1, self.before, self.plus)
            self.got(0, 3, self.after, self.minus)
            self.got(0, 4, self.across, self.plus)
            self.got(1, 5, self.across, self.minus)

    class Scatter:
        def __init__(self, axis, block, land):
            self.plus, self.minus = to[(axis, 1)], to[(axis, -1)]
            p = place[axis]
            self.block, self.land = block, land
            self.here, self.after, self.across, self.before = p, nxt(p, 1), nxt(p, 2), nxt(p, 3)
            self.base = reserve(6)

        def go(self, half, index, owner, target):
            send(self.block(owner, half), self.land(index), self.base + index, target)

        def got(self, index, target):
            arrived(self.land(index), self.base + index, target)

        def add(self, owner, half, index):
            mine = self.block(owner, half)
            mine[...] = (mine[...].astype(F32) + self.land(index)[...].astype(F32)).astype(BF)

        def start(self):
            self.go(0, 0, self.across, self.plus)
            self.go(1, 1, self.across, self.minus)
            self.go(1, 2, self.after, self.plus)
            self.go(0, 3, self.before, self.minus)

        def mid(self):
            self.got(0, self.plus)
            self.add(self.after, 0, 0)
            self.go(0, 4, self.after, self.plus)
            self.got(1, self.minus)
            self.add(self.before, 1, 1)
            self.go(1, 5, self.before, self.minus)

        def end(self, store):
            for index in (2, 3, 4, 5):
                self.got(index, self.plus if index in (2, 4) else self.minus)
            for half, parts in ((0, (3, 4)), (1, (2, 5))):
                total = self.block(self.here, half)[...].astype(F32)
                for index in parts:
                    total = total + self.land(index)[...].astype(F32)
                store(half, total)

    def gathers(weight):
        cols_a, cols_b = COLS
        one_a = Gather("y", lambda p, h: weight.at[z, rows_at(p * 128 + h * 64, 64), cols_a])
        one_b = Gather("z", lambda p, h: weight.at[p, rows_at(y * 128 + h * 64, 64), cols_b])
        two_a = Gather("z", lambda p, h: weight.at[p, pl.ds(h * 256, 256), cols_a])
        two_b = Gather("y", lambda p, h: weight.at[pl.ds(h * 2, 2), rows_at(p * 128, 128), cols_b])
        return one_a, one_b, two_a, two_b

    class GradSum:
        def __init__(self, grad, which, accum, out):
            cols_a, cols_b = COLS
            self.grad, self.accum, self.out = grad, accum, out
            self.one_a = Scatter(
                "z", lambda p, h: grad.at[p, pl.ds(h * 256, 256), cols_a],
                lambda i: land_z.at[which, i],
            )
            self.one_b = Scatter(
                "y", lambda p, h: grad.at[pl.ds(h * 2, 2), rows_at(p * 128, 128), cols_b],
                lambda i: land_y.at[which, i],
            )
            self.two_a = Scatter(
                "y", lambda p, h: grad.at[z, rows_at(p * 128 + h * 64, 64), cols_a],
                lambda i: land_2.at[which, 0, i],
            )
            self.two_b = Scatter(
                "z", lambda p, h: grad.at[p, rows_at(y * 128 + h * 64, 64), cols_b],
                lambda i: land_2.at[which, 1, i],
            )

        def start(self):
            self.one_a.start()
            self.one_b.start()

        def mid(self):
            self.one_a.mid()
            self.one_b.mid()

        def turn(self):
            for ring in (self.one_a, self.one_b):
                def keep(half, total, ring=ring):
                    ring.block(ring.here, half)[...] = total.astype(BF)
                ring.end(keep)
            self.two_a.start()
            self.two_b.start()

        def mid_2(self):
            self.two_a.mid()
            self.two_b.mid()

        def end(self):
            for ring, cols in ((self.two_a, COLS[0]), (self.two_b, COLS[1])):
                def keep(half, total, cols=cols):
                    rows = pl.ds(half * 64, 64)
                    self.out[rows, cols] = self.accum[rows, cols] + 0.0078125 * total
                ring.end(keep)

    class TokenSum:
        def __init__(self, part, which, out):
            self.part, self.which, self.out = part, which, out
            self.base = reserve(4)
            self.order = (nxt(x, 2), nxt(x, 1), nxt(x, 3), x)
            self.ring = Scatter(
                "x", lambda p, h: part.at[p, rows_at(core * 128 + h * 64, 64), :],
                lambda i: land_x.at[which, i],
            )

        def offer(self, step):
            chunk = self.order[step]
            send(
                self.part.at[chunk, rows_at((1 - core) * 128, 128), :],
                land_pair.at[self.which, step],
                self.base + step,
                to["pair"],
            )

        def join(self, step):
            chunk = self.order[step]
            landed = land_pair.at[self.which, step]
            arrived(landed, self.base + step, to["pair"])
            mine = self.part.at[chunk, rows_at(core * 128, 128), :]
            mine[...] = (mine[...].astype(F32) + landed[...].astype(F32)).astype(BF)

        def end(self):
            def keep(half, total):
                self.out[pl.ds(half * 64, 64), :] = total.astype(BF)
            self.ring.end(keep)

    loads = [
        pltpu.make_async_copy(up_hbm, up_w.at[z, rows_at(y * 128, 128), :], load_sem.at[0]),
        pltpu.make_async_copy(down_hbm, down_w.at[z, rows_at(y * 128, 128), :], load_sem.at[1]),
        pltpu.make_async_copy(saved_hbm, saved, load_sem.at[2]),
        pltpu.make_async_copy(upstream_hbm, upstream, load_sem.at[3]),
        pltpu.make_async_copy(fresh_hbm, fresh, load_sem.at[4]),
        pltpu.make_async_copy(accum_up_hbm, accum_up, load_sem.at[5]),
        pltpu.make_async_copy(accum_down_hbm, accum_down, load_sem.at[6]),
    ]
    for load in loads:
        load.start()

    barrier = pltpu.get_barrier_semaphore()
    for target in to.values():
        pl.semaphore_signal(barrier, inc=1, device_id=target, device_id_type=MESH)
    pl.semaphore_wait(barrier, len(to))

    up_1a, up_1b, up_2a, up_2b = gathers(up_w)
    down_1a, down_1b, down_2a, down_2b = gathers(down_w)
    down_sum = GradSum(grad_down, 0, accum_down, accum_down_out)
    up_sum = GradSum(grad_up, 1, accum_up, accum_up_out)
    fresh_sum = TokenSum(fresh, 0, fresh_out)
    saved_sum = TokenSum(saved, 1, saved_grad)

    def forward(rows, store):
        def step(j, carry):
            i, n = j // 2, j % 2
            tile = rows[pl.ds(i * 2, 2)].reshape(512, 2048)
            cols = rows_at(n * 512, 512)
            pre = jnp.dot(
                tile, up_w[:, :, cols].reshape(2048, 512), preferred_element_type=F32
            )
            store(rows_at(i * 512, 512), cols, jnp.maximum(pre, 0.0))
            return carry
        lax.fori_loop(0, 4, step, 0)

    def keep_saved(at, cols, active):
        saved_active[at, cols] = active.astype(BF)
        saved_hidden[at, cols] = (active * active).astype(BF)

    def keep_fresh(at, cols, active):
        fresh_hidden[at, cols] = (active * active).astype(BF)

    def weight_grad(left, right, grad):
        def step(j, carry):
            cols = rows_at(j * 512, 512)
            tile = left(cols)
            total = lax.dot_general(
                tile, right[...], (((0,), (0,)), ((), ())), preferred_element_type=F32
            )
            grad[j] = total.astype(BF)
            return carry
        lax.fori_loop(0, 4, step, 0)

    def output_chunk(hidden, weight, part, chunk):
        def step(n, carry):
            total = lax.dot_general(
                hidden[rows_at(chunk * 256, 256), :], weight[n],
                (((1,), (1,)), ((), ())), preferred_element_type=F32,
            )
            part[chunk, :, rows_at(n * 512, 512)] = total.astype(BF)
            return carry
        lax.fori_loop(0, 4, step, 0)

    loads[0].wait()
    loads[1].wait()
    up_1a.start()
    up_1b.start()
    down_1a.start()
    down_1b.start()
    up_1a.mid()
    up_1b.mid()
    up_1a.end()
    up_1b.end()
    up_2a.start()
    up_2b.start()
    down_1a.mid()
    down_1b.mid()
    down_1a.end()
    down_1b.end()
    up_2a.mid()
    up_2b.mid()
    down_2a.start()
    down_2b.start()
    for load in loads[2:]:
        load.wait()
    up_2a.end()
    up_2b.end()

    forward(saved, keep_saved)
    down_2a.mid()
    down_2b.mid()
    weight_grad(lambda cols: upstream[:, cols], saved_hidden, grad_down)
    down_sum.start()
    forward(fresh, keep_fresh)
    down_2a.end()
    down_2b.end()

    for step in range(4):
        output_chunk(fresh_hidden, down_w, fresh, fresh_sum.order[step])
        fresh_sum.offer(step)
        if step == 1:
            down_sum.mid()
    for step in range(4):
        fresh_sum.join(step)
    fresh_sum.ring.start()

    def backward(j, carry):
        i, n = j // 2, j % 2
        at, cols = rows_at(i * 512, 512), rows_at(n * 512, 512)
        hidden_grad = jnp.dot(
            upstream[at, :], down_w[:, :, cols].reshape(2048, 512), preferred_element_type=F32
        )
        pre_grad[at, cols] = (2.0 * saved_active[at, cols].astype(F32) * hidden_grad).astype(BF)
        return carry
    lax.fori_loop(0, 4, backward, 0)
    fresh_sum.ring.mid()
    down_sum.turn()
    weight_grad(lambda cols: saved[:, :, cols].reshape(1024, 512), pre_grad, grad_up)
    up_sum.start()
    down_sum.mid_2()

    for step in range(4):
        output_chunk(pre_grad, up_w, saved, saved_sum.order[step])
        saved_sum.offer(step)
    fresh_sum.end()
    for step in range(4):
        saved_sum.join(step)
    saved_sum.ring.start()
    up_sum.mid()
    down_sum.end()
    saved_sum.ring.mid()
    up_sum.turn()
    up_sum.mid_2()
    saved_sum.end()
    up_sum.end()
    for copy in sent:
        copy.wait_send()


def body(fresh_rows, saved_rows, upstream_grad, proj_up, proj_down, accum_up, accum_down):
    anywhere = pl.BlockSpec(memory_space=pl.ANY)
    inside = pl.BlockSpec(memory_space=pltpu.VMEM)
    shape = jax.ShapeDtypeStruct
    return pl.pallas_call(
        kernel,
        out_shape=(
            shape((128, 2048), BF), shape((128, 2048), BF),
            shape((128, 1024), F32), shape((128, 1024), F32),
        ),
        in_specs=[anywhere] * 7,
        out_specs=(inside,) * 4,
        scratch_shapes=[
            pltpu.VMEM((4, 256, 2048), BF),
            pltpu.VMEM((4, 256, 2048), BF),
            pltpu.VMEM((1024, 2048), BF),
            pltpu.VMEM((4, 512, 1024), BF),
            pltpu.VMEM((4, 512, 1024), BF),
            pltpu.VMEM((128, 1024), F32),
            pltpu.VMEM((128, 1024), F32),
            pltpu.VMEM((1024, 1024), BF),
            pltpu.VMEM((1024, 1024), BF),
            pltpu.VMEM((1024, 1024), BF),
            pltpu.VMEM((1024, 1024), BF),
            pltpu.VMEM((4, 512, 1024), BF),
            pltpu.VMEM((4, 512, 1024), BF),
            pltpu.VMEM((2, 6, 256, 512), BF),
            pltpu.VMEM((2, 6, 2, 128, 512), BF),
            pltpu.VMEM((2, 2, 6, 64, 512), BF),
            pltpu.VMEM((2, 4, 128, 2048), BF),
            pltpu.VMEM((2, 6, 64, 2048), BF),
            pltpu.SemaphoreType.DMA((N_MSG,)),
            pltpu.SemaphoreType.DMA((N_MSG,)),
            pltpu.SemaphoreType.DMA((7,)),
        ],
        compiler_params=pltpu.CompilerParams(
            collective_id=0, has_side_effects=True, vmem_limit_bytes=67043328
        ),
        cost_estimate=pl.CostEstimate(
            flops=30064771072, bytes_accessed=32 * 1024 * 1024, transcendentals=0
        ),
    )(
        fresh_rows.reshape(4, 256, 2048), saved_rows.reshape(4, 256, 2048), upstream_grad,
        proj_up, proj_down, accum_up, accum_down,
    )


def solution(mesh):
    in_specs = (
        P("fs", None),
        P("fs", None),
        P("fs", None),
        P("fs", "tp"),
        P("fs", "tp"),
        P("fs", "tp"),
        P("fs", "tp"),
    )
    out_specs = (P(("fs", "tp"), None), P(("fs", "tp"), None), P("fs", "tp"), P("fs", "tp"))
    return jax.shard_map(body, mesh=mesh, in_specs=in_specs, out_specs=out_specs, check_vma=False)
```

```python
import jax
import jax.numpy as jnp
from jax import lax
from jax.experimental import pallas as pl
from jax.experimental.pallas import tpu as pltpu
from jax.sharding import PartitionSpec as P

MESH = pl.DeviceIdType.MESH
BF = jnp.bfloat16
F32 = jnp.float32
COLS = (slice(0, 512), slice(512, 1024))
N_GATHER = 48
N_GRADS = 48
N_X = 20
N_MSG = N_GATHER + N_GRADS + N_X


def rows_at(start, size):
    return pl.ds(pl.multiple_of(start, size), size)


def kernel(
    fresh_hbm, saved_hbm, upstream_hbm, up_hbm, down_hbm, accum_up_hbm, accum_down_hbm,
    fresh_out, saved_grad, accum_up_out, accum_down_out,
    fresh, saved, upstream, up_w, down_w, accum_up, accum_down,
    saved_t, upstream_t, fresh_hidden, saved_active, saved_hidden, pre_grad, grad_down,
    land_z, land_y, land_2, land_pair, land_x,
    send_sem, recv_sem, load_sem,
):
    fs, tp = lax.axis_index("fs"), lax.axis_index("tp")
    z, y, x, core = fs // 4, fs % 4, tp // 2, tp % 2

    def nxt(p, by):
        return lax.rem(p + by, 4)

    to = {
        ("y", 1): (z * 4 + nxt(y, 1), tp),
        ("y", -1): (z * 4 + nxt(y, 3), tp),
        ("z", 1): (nxt(z, 1) * 4 + y, tp),
        ("z", -1): (nxt(z, 3) * 4 + y, tp),
        ("x", 1): (fs, nxt(x, 1) * 2 + core),
        ("x", -1): (fs, nxt(x, 3) * 2 + core),
        "pair": (fs, x * 2 + 1 - core),
    }
    place = {"y": y, "z": z, "x": x}
    used = [0]
    sent = []

    def reserve(count):
        used[0] += count
        return used[0] - count

    def message(src, dst, index, target):
        return pltpu.make_async_remote_copy(
            src_ref=src,
            dst_ref=dst,
            send_sem=send_sem.at[index],
            recv_sem=recv_sem.at[index],
            device_id=target,
            device_id_type=MESH,
        )

    def send(src, dst, index, target):
        copy = message(src, dst, index, target)
        copy.start()
        sent.append(copy)

    def arrived(dst, index, target):
        message(dst, dst, index, target).wait_recv()

    class Gather:
        def __init__(self, axis, block):
            self.plus, self.minus = to[(axis, 1)], to[(axis, -1)]
            p = place[axis]
            self.block = block
            self.here, self.after, self.across, self.before = p, nxt(p, 1), nxt(p, 2), nxt(p, 3)
            self.base = reserve(6)

        def go(self, half, index, owner, target):
            part = self.block(owner, half)
            send(part, part, self.base + index, target)

        def got(self, half, index, owner, target):
            arrived(self.block(owner, half), self.base + index, target)

        def start(self):
            self.go(0, 0, self.here, self.plus)
            self.go(1, 2, self.here, self.minus)

        def rest(self):
            self.go(1, 1, self.here, self.plus)
            self.go(0, 3, self.here, self.minus)

        def mid(self):
            self.got(0, 0, self.before, self.plus)
            self.go(0, 4, self.before, self.plus)
            self.got(1, 2, self.after, self.minus)
            self.go(1, 5, self.after, self.minus)

        def end(self):
            self.got(1, 1, self.before, self.plus)
            self.got(0, 3, self.after, self.minus)
            self.got(0, 4, self.across, self.plus)
            self.got(1, 5, self.across, self.minus)

    class Scatter:
        def __init__(self, axis, block, land):
            self.plus, self.minus = to[(axis, 1)], to[(axis, -1)]
            p = place[axis]
            self.block, self.land = block, land
            self.here, self.after, self.across, self.before = p, nxt(p, 1), nxt(p, 2), nxt(p, 3)
            self.base = reserve(6)

        def go(self, half, index, owner, target):
            send(self.block(owner, half), self.land(index), self.base + index, target)

        def got(self, index, target):
            arrived(self.land(index), self.base + index, target)

        def add(self, owner, half, index):
            mine = self.block(owner, half)
            mine[...] = (mine[...].astype(F32) + self.land(index)[...].astype(F32)).astype(BF)

        def start(self):
            self.go(0, 0, self.across, self.plus)
            self.go(1, 1, self.across, self.minus)

        def rest(self):
            self.go(1, 2, self.after, self.plus)
            self.go(0, 3, self.before, self.minus)

        def mid(self):
            self.got(0, self.plus)
            self.add(self.after, 0, 0)
            self.go(0, 4, self.after, self.plus)
            self.got(1, self.minus)
            self.add(self.before, 1, 1)
            self.go(1, 5, self.before, self.minus)

        def end(self, store):
            for index in (2, 3, 4, 5):
                self.got(index, self.plus if index in (2, 4) else self.minus)
            for half, parts in ((0, (3, 4)), (1, (2, 5))):
                total = self.block(self.here, half)[...].astype(F32)
                for index in parts:
                    total = total + self.land(index)[...].astype(F32)
                store(half, total)

    def gathers(weight):
        cols_a, cols_b = COLS
        one_a = Gather("y", lambda p, h: weight.at[z, rows_at(p * 128 + h * 64, 64), cols_a])
        one_b = Gather("z", lambda p, h: weight.at[p, rows_at(y * 128 + h * 64, 64), cols_b])
        two_a = Gather("z", lambda p, h: weight.at[p, pl.ds(h * 256, 256), cols_a])
        two_b = Gather("y", lambda p, h: weight.at[pl.ds(h * 2, 2), rows_at(p * 128, 128), cols_b])
        return one_a, one_b, two_a, two_b

    class GradSum:
        def __init__(self, grad, which, accum, out):
            cols_a, cols_b = COLS
            self.grad, self.accum, self.out = grad, accum, out
            self.one_a = Scatter(
                "z", lambda p, h: grad.at[p, pl.ds(h * 256, 256), cols_a],
                lambda i: land_z.at[which, i],
            )
            self.one_b = Scatter(
                "y", lambda p, h: grad.at[pl.ds(h * 2, 2), rows_at(p * 128, 128), cols_b],
                lambda i: land_y.at[which, i],
            )
            self.two_a = Scatter(
                "y", lambda p, h: grad.at[z, rows_at(p * 128 + h * 64, 64), cols_a],
                lambda i: land_2.at[which, 0, i],
            )
            self.two_b = Scatter(
                "z", lambda p, h: grad.at[p, rows_at(y * 128 + h * 64, 64), cols_b],
                lambda i: land_2.at[which, 1, i],
            )

        def start(self):
            self.one_a.start()
            self.one_b.start()

        def rest(self):
            self.one_a.rest()
            self.one_b.rest()

        def mid(self):
            self.one_a.mid()
            self.one_b.mid()

        def turn(self):
            for ring in (self.one_a, self.one_b):
                def keep(half, total, ring=ring):
                    ring.block(ring.here, half)[...] = total.astype(BF)
                ring.end(keep)
            self.two_a.start()
            self.two_b.start()
            self.two_a.rest()
            self.two_b.rest()

        def mid_2(self):
            self.two_a.mid()
            self.two_b.mid()

        def end(self):
            for ring, cols in ((self.two_a, COLS[0]), (self.two_b, COLS[1])):
                def keep(half, total, cols=cols):
                    rows = pl.ds(half * 64, 64)
                    self.out[rows, cols] = self.accum[rows, cols] + 0.0078125 * total
                ring.end(keep)

    class TokenSum:
        def __init__(self, part, which, out):
            self.part, self.which, self.out = part, which, out
            self.base = reserve(4)
            self.order = (nxt(x, 2), nxt(x, 1), nxt(x, 3), x)
            self.ring = Scatter(
                "x", lambda p, h: part.at[p, rows_at(core * 128 + h * 64, 64), :],
                lambda i: land_x.at[which, i],
            )

        def offer(self, step):
            chunk = self.order[step]
            send(
                self.part.at[chunk, rows_at((1 - core) * 128, 128), :],
                land_pair.at[self.which, step],
                self.base + step,
                to["pair"],
            )

        def join(self, step):
            chunk = self.order[step]
            landed = land_pair.at[self.which, step]
            arrived(landed, self.base + step, to["pair"])
            mine = self.part.at[chunk, rows_at(core * 128, 128), :]
            mine[...] = (mine[...].astype(F32) + landed[...].astype(F32)).astype(BF)

        def end(self):
            def keep(half, total):
                self.out[pl.ds(half * 64, 64), :] = total.astype(BF)
            self.ring.end(keep)

    loads = [
        pltpu.make_async_copy(up_hbm, up_w.at[z, rows_at(y * 128, 128), :], load_sem.at[0]),
        pltpu.make_async_copy(down_hbm, down_w.at[z, rows_at(y * 128, 128), :], load_sem.at[1]),
        pltpu.make_async_copy(saved_hbm, saved, load_sem.at[2]),
        pltpu.make_async_copy(upstream_hbm, upstream, load_sem.at[3]),
        pltpu.make_async_copy(fresh_hbm, fresh, load_sem.at[4]),
        pltpu.make_async_copy(accum_up_hbm, accum_up, load_sem.at[5]),
        pltpu.make_async_copy(accum_down_hbm, accum_down, load_sem.at[6]),
    ]
    for load in loads:
        load.start()

    barrier = pltpu.get_barrier_semaphore()
    for target in to.values():
        pl.semaphore_signal(barrier, inc=1, device_id=target, device_id_type=MESH)
    pl.semaphore_wait(barrier, len(to))

    up_1a, up_1b, up_2a, up_2b = gathers(up_w)
    down_1a, down_1b, down_2a, down_2b = gathers(down_w)
    grad_up = upstream_t
    down_sum = GradSum(grad_down, 0, accum_down, accum_down_out)
    up_sum = GradSum(grad_up, 1, accum_up, accum_up_out)
    fresh_sum = TokenSum(fresh, 0, fresh_out)
    saved_sum = TokenSum(saved, 1, saved_grad)

    def turned(rows, out):
        def step(i, carry):
            out[:, :, rows_at(i * 256, 256)] = rows[i].T.reshape(4, 512, 256)
            return carry
        lax.fori_loop(0, 4, step, 0)

    def forward(rows, store):
        def step(j, carry):
            i, n = j // 2, j % 2
            tile = rows[pl.ds(i * 2, 2)].reshape(512, 2048)
            cols = rows_at(n * 512, 512)
            pre = jnp.dot(
                tile, up_w[:, :, cols].reshape(2048, 512), preferred_element_type=F32
            )
            store(rows_at(i * 512, 512), cols, jnp.maximum(pre, 0.0))
            return carry
        lax.fori_loop(0, 4, step, 0)

    def keep_saved(at, cols, active):
        saved_active[at, cols] = active.astype(BF)
        saved_hidden[at, cols] = (active * active).astype(BF)

    def keep_fresh(at, cols, active):
        fresh_hidden[at, cols] = (active * active).astype(BF)

    def backward():
        def step(j, carry):
            i, n = j // 2, j % 2
            at, cols = rows_at(i * 512, 512), rows_at(n * 512, 512)
            hidden_grad = jnp.dot(
                upstream[pl.ds(i * 2, 2)].reshape(512, 2048),
                down_w[:, :, cols].reshape(2048, 512), preferred_element_type=F32,
            )
            pre_grad[at, cols] = (2.0 * saved_active[at, cols].astype(F32) * hidden_grad).astype(BF)
            return carry
        lax.fori_loop(0, 4, step, 0)

    def grad_piece(left, right, out, by):
        plane, block = nxt(z, by), rows_at(nxt(y, by) * 128, 128)
        total = jnp.dot(left[plane], right[:, COLS[0]], preferred_element_type=F32)
        out[plane, :, COLS[0]] = total.astype(BF)
        total = jnp.dot(
            left[:, block, :].reshape(512, 1024), right[:, COLS[1]], preferred_element_type=F32
        )
        out[:, block, COLS[1]] = total.astype(BF).reshape(4, 128, 512)

    def output_pair(hidden, weight, part, chunks):
        left = jnp.concatenate([hidden[rows_at(c * 256, 256), :] for c in chunks], axis=0)
        def step(n, carry):
            total = lax.dot_general(
                left, weight[n], (((1,), (1,)), ((), ())), preferred_element_type=F32
            ).astype(BF)
            part[chunks[0], :, rows_at(n * 512, 512)] = total[:256]
            part[chunks[1], :, rows_at(n * 512, 512)] = total[256:]
            return carry
        lax.fori_loop(0, 4, step, 0)

    loads[0].wait()
    loads[1].wait()
    for ring in (up_1a, up_1b):
        ring.start()
    for ring in (up_1a, up_1b):
        ring.rest()
    for ring in (up_1a, up_1b):
        ring.mid()
    for ring in (down_1a, down_1b):
        ring.start()
        ring.rest()
    for load in loads[2:]:
        load.wait()
    for ring in (up_1a, up_1b):
        ring.end()
    for ring in (up_2a, up_2b):
        ring.start()
    for ring in (down_1a, down_1b):
        ring.mid()
    for ring in (up_2a, up_2b):
        ring.rest()
    turned(upstream, upstream_t)
    for ring in (up_2a, up_2b):
        ring.mid()
    for ring in (down_1a, down_1b):
        ring.end()
    for ring in (down_2a, down_2b):
        ring.start()
        ring.rest()
    turned(saved, saved_t)
    for ring in (up_2a, up_2b):
        ring.end()

    forward(saved, keep_saved)
    for ring in (down_2a, down_2b):
        ring.mid()
    for by in (2, 1, 3, 0):
        grad_piece(upstream_t, saved_hidden, grad_down, by)
    down_sum.start()
    down_sum.rest()
    forward(fresh, keep_fresh)
    for ring in (down_2a, down_2b):
        ring.end()

    output_pair(fresh_hidden, down_w, fresh, fresh_sum.order[:2])
    fresh_sum.offer(0)
    fresh_sum.offer(1)
    output_pair(fresh_hidden, down_w, fresh, fresh_sum.order[2:])
    fresh_sum.offer(2)
    fresh_sum.offer(3)
    fresh_sum.join(0)
    fresh_sum.ring.start()
    fresh_sum.join(1)
    down_sum.mid()
    fresh_sum.join(2)
    fresh_sum.ring.rest()
    backward()
    fresh_sum.join(3)
    fresh_sum.ring.mid()
    grad_piece(saved_t, pre_grad, grad_up, 2)
    up_sum.start()
    grad_piece(saved_t, pre_grad, grad_up, 1)
    down_sum.turn()
    grad_piece(saved_t, pre_grad, grad_up, 3)
    up_sum.rest()
    grad_piece(saved_t, pre_grad, grad_up, 0)
    output_pair(pre_grad, up_w, saved, saved_sum.order[:2])
    saved_sum.offer(0)
    saved_sum.offer(1)
    up_sum.mid()
    output_pair(pre_grad, up_w, saved, saved_sum.order[2:])
    saved_sum.offer(2)
    saved_sum.offer(3)
    saved_sum.join(0)
    saved_sum.ring.start()
    saved_sum.join(1)
    saved_sum.join(2)
    saved_sum.ring.rest()
    saved_sum.join(3)
    down_sum.mid_2()
    fresh_sum.end()
    saved_sum.ring.mid()
    up_sum.turn()
    down_sum.end()
    up_sum.mid_2()
    saved_sum.end()
    up_sum.end()
    for copy in sent:
        copy.wait_send()


def settle(a, b, c, d, out_a, out_b, out_c, out_d):
    out_a[...] = a[...]
    out_b[...] = b[...]
    out_c[...] = c[...]
    out_d[...] = d[...]


def body(fresh_rows, saved_rows, upstream_grad, proj_up, proj_down, accum_up, accum_down):
    anywhere = pl.BlockSpec(memory_space=pl.ANY)
    inside = pl.BlockSpec(memory_space=pltpu.VMEM)
    shape = jax.ShapeDtypeStruct
    results = pl.pallas_call(
        kernel,
        out_shape=(
            shape((128, 2048), BF), shape((128, 2048), BF),
            shape((128, 1024), F32), shape((128, 1024), F32),
        ),
        in_specs=[anywhere] * 7,
        out_specs=(inside,) * 4,
        scratch_shapes=[
            pltpu.VMEM((4, 256, 2048), BF),
            pltpu.VMEM((4, 256, 2048), BF),
            pltpu.VMEM((4, 256, 2048), BF),
            pltpu.VMEM((4, 512, 1024), BF),
            pltpu.VMEM((4, 512, 1024), BF),
            pltpu.VMEM((128, 1024), F32),
            pltpu.VMEM((128, 1024), F32),
            pltpu.VMEM((4, 512, 1024), BF),
            pltpu.VMEM((4, 512, 1024), BF),
            pltpu.VMEM((1024, 1024), BF),
            pltpu.VMEM((1024, 1024), BF),
            pltpu.VMEM((1024, 1024), BF),
            pltpu.VMEM((1024, 1024), BF),
            pltpu.VMEM((4, 512, 1024), BF),
            pltpu.VMEM((2, 6, 256, 512), BF),
            pltpu.VMEM((2, 6, 2, 128, 512), BF),
            pltpu.VMEM((2, 2, 6, 64, 512), BF),
            pltpu.VMEM((2, 4, 128, 2048), BF),
            pltpu.VMEM((2, 6, 64, 2048), BF),
            pltpu.SemaphoreType.DMA((N_MSG,)),
            pltpu.SemaphoreType.DMA((N_MSG,)),
            pltpu.SemaphoreType.DMA((7,)),
        ],
        compiler_params=pltpu.CompilerParams(
            collective_id=0, has_side_effects=True, vmem_limit_bytes=67043328
        ),
        cost_estimate=pl.CostEstimate(
            flops=30064771072, bytes_accessed=32 * 1024 * 1024, transcendentals=0
        ),
    )(
        fresh_rows.reshape(4, 256, 2048), saved_rows.reshape(4, 256, 2048),
        upstream_grad.reshape(4, 256, 2048),
        proj_up, proj_down, accum_up, accum_down,
    )
    return pl.pallas_call(
        settle,
        out_shape=tuple(shape(r.shape, r.dtype) for r in results),
        in_specs=[inside] * 4,
        out_specs=(inside,) * 4,
    )(*results)


def solution(mesh):
    in_specs = (
        P("fs", None),
        P("fs", None),
        P("fs", None),
        P("fs", "tp"),
        P("fs", "tp"),
        P("fs", "tp"),
        P("fs", "tp"),
    )
    out_specs = (P(("fs", "tp"), None), P(("fs", "tp"), None), P("fs", "tp"), P("fs", "tp"))
    return jax.shard_map(body, mesh=mesh, in_specs=in_specs, out_specs=out_specs, check_vma=False)
```

```python
import jax
import jax.numpy as jnp
from jax import lax
from jax.experimental import pallas as pl
from jax.experimental.pallas import tpu as pltpu
from jax.sharding import PartitionSpec as P

MESH = pl.DeviceIdType.MESH
BF = jnp.bfloat16
F32 = jnp.float32
COLS = (slice(0, 512), slice(512, 1024))
GROUPS = tuple((slice(q, q + 256), slice(q + 512, q + 768)) for q in (0, 256))
N_RINGS = 12 + 16 + 2


def rows_at(start, size):
    return pl.ds(pl.multiple_of(start, size), size)


def kernel(
    fresh_hbm, saved_hbm, upstream_hbm, up_hbm, down_hbm, accum_up_hbm, accum_down_hbm,
    fresh_out, saved_grad, accum_up_out, accum_down_out,
    fresh, saved, upstream, up_w, down_w, accum_up, accum_down,
    saved_t, upstream_t, fresh_hidden, saved_active, saved_hidden, pre_grad, grad_down,
    land_z, land_y, land_2, land_pair, land_x,
    send_sem, recv_sem, load_sem,
):
    fs, tp = lax.axis_index("fs"), lax.axis_index("tp")
    z, y, x, core = fs // 4, fs % 4, tp // 2, tp % 2

    def nxt(p, by):
        return lax.rem(p + by, 4)

    to = {
        ("y", 1): (z * 4 + nxt(y, 1), tp),
        ("y", -1): (z * 4 + nxt(y, 3), tp),
        ("z", 1): (nxt(z, 1) * 4 + y, tp),
        ("z", -1): (nxt(z, 3) * 4 + y, tp),
        ("x", 1): (fs, nxt(x, 1) * 2 + core),
        ("x", -1): (fs, nxt(x, 3) * 2 + core),
        "pair": (fs, x * 2 + 1 - core),
    }
    place = {"y": y, "z": z, "x": x}
    used = [0]
    part_of = (slice(None), pl.ds(0, 480))
    bulks = (up_w.at[part_of], down_w.at[part_of], land_z, land_y, land_2, land_x, land_pair)

    def reserve(count):
        used[0] += count
        return used[0] - count

    def message(src, dst, sends, receives, target):
        return pltpu.make_async_remote_copy(
            src_ref=src,
            dst_ref=dst,
            send_sem=send_sem.at[sends],
            recv_sem=recv_sem.at[receives],
            device_id=target,
            device_id_type=MESH,
        )

    class Ring:
        def __init__(self, axis, pool):
            self.plus, self.minus = to[(axis, 1)], to[(axis, -1)]
            p = place[axis]
            self.here, self.after, self.across, self.before = p, nxt(p, 1), nxt(p, 2), nxt(p, 3)
            self.out, self.into = pool, reserve(3)

        def push(self, src, dst, slot, target):
            message(src, dst, self.out, self.into + slot, target).start()

        def got(self, dst, slot):
            message(dst, dst, self.out, self.into + slot, self.plus).wait_recv()

    class Gather(Ring):
        def __init__(self, axis, block, two, pool):
            super().__init__(axis, pool)
            self.block, self.two = block, two

        def go(self, half, slot, owner, target):
            part = self.block(owner, half)
            self.push(part, part, slot, target)

        def start(self):
            self.go(0, 0, self.here, self.plus)
            self.go(1, 1, self.here, self.minus)

        def rest(self):
            self.go(1, 2, self.here, self.plus)
            self.go(0, 2, self.here, self.minus)

        def mid(self):
            self.got(self.block(self.before, 0), 0)
            self.go(0, 2, self.before, self.plus)
            self.got(self.block(self.after, 1), 1)
            self.go(1, 2, self.after, self.minus)

        def end(self):
            self.got(self.two, 2)

    class Scatter(Ring):
        def __init__(self, axis, block, land, pool):
            super().__init__(axis, pool)
            self.block, self.land = block, land

        def go(self, half, slot, index, owner, target):
            self.push(self.block(owner, half), self.land.at[index], slot, target)

        def add(self, owner, half, index):
            mine = self.block(owner, half)
            mine[...] = (mine[...].astype(F32) + self.land[index].astype(F32)).astype(BF)

        def start(self):
            self.go(0, 0, 0, self.across, self.plus)
            self.go(1, 1, 1, self.across, self.minus)

        def rest(self):
            self.go(1, 2, 2, self.after, self.plus)
            self.go(0, 2, 3, self.before, self.minus)

        def mid(self):
            self.got(self.land.at[0], 0)
            self.add(self.after, 0, 0)
            self.go(0, 2, 4, self.after, self.plus)
            self.got(self.land.at[1], 1)
            self.add(self.before, 1, 1)
            self.go(1, 2, 5, self.before, self.minus)

        def end(self, store):
            self.got(self.land.at[pl.ds(2, 4)], 2)
            for half, parts in ((0, (3, 4)), (1, (2, 5))):
                total = self.block(self.here, half)[...].astype(F32)
                for index in parts:
                    total = total + self.land[index].astype(F32)
                store(half, total)

    class Both:
        def __init__(self, *rings):
            self.rings = rings

        def __getattr__(self, step):
            def run():
                for ring in self.rings:
                    getattr(ring, step)()
            return run

    def gather_1(w, pool):
        a, b = COLS
        return Both(
            Gather(
                "y", lambda p, h: w.at[z, rows_at(p * 128 + h * 64, 64), a],
                w.at[0, pl.ds(0, 256), a], pool,
            ),
            Gather(
                "z", lambda p, h: w.at[p, rows_at(y * 128 + h * 64, 64), b],
                w.at[0, pl.ds(0, 256), b], pool,
            ),
        )

    def gather_2(w, q, pool):
        a, b = GROUPS[q]
        return Both(
            Gather(
                "z", lambda p, h: w.at[p, pl.ds(h * 256, 256), a],
                w.at[pl.ds(0, 2), :, a], pool,
            ),
            Gather(
                "y", lambda p, h: w.at[pl.ds(h * 2, 2), rows_at(p * 128, 128), b],
                w.at[:, pl.ds(0, 256), b], pool,
            ),
        )

    class GradSum:
        def __init__(self, grad, which, q, accum, out):
            a, b = GROUPS[q]
            self.q, self.accum, self.out = q, accum, out
            self.one = (
                Scatter(
                    "z", lambda p, h: grad.at[p, pl.ds(h * 256, 256), a],
                    land_z.at[which, q], 2,
                ),
                Scatter(
                    "y", lambda p, h: grad.at[pl.ds(h * 2, 2), rows_at(p * 128, 128), b],
                    land_y.at[which, q], 3,
                ),
            )
            self.two = (
                Scatter(
                    "y", lambda p, h: grad.at[z, rows_at(p * 128 + h * 64, 64), a],
                    land_2.at[which, q, 0], 4,
                ),
                Scatter(
                    "z", lambda p, h: grad.at[p, rows_at(y * 128 + h * 64, 64), b],
                    land_2.at[which, q, 1], 4,
                ),
            )

        def start(self):
            for ring in self.one:
                ring.start()
            for ring in self.one:
                ring.rest()

        def mid(self):
            for ring in self.one:
                ring.mid()

        def turn(self):
            for ring, after in zip(self.one, self.two):
                def keep(half, total, ring=ring):
                    ring.block(ring.here, half)[...] = total.astype(BF)
                ring.end(keep)
                after.start()
                after.rest()

        def mid_2(self):
            for ring in self.two:
                ring.mid()

        def end(self):
            for ring, cols in zip(self.two, GROUPS[self.q]):
                def keep(half, total, cols=cols):
                    rows = pl.ds(half * 64, 64)
                    self.out[rows, cols] = self.accum[rows, cols] + 0.0078125 * total
                ring.end(keep)

    class TokenSum:
        def __init__(self, part, which, out):
            self.part, self.which, self.out = part, which, out
            self.receives = reserve(4)
            self.order = (nxt(x, 2), nxt(x, 1), nxt(x, 3), x)
            self.ring = Scatter(
                "x", lambda p, h: part.at[p, rows_at(core * 128 + h * 64, 64), :],
                land_x.at[which], 5,
            )

        def pair(self, src, step):
            return message(
                src, land_pair.at[self.which, step],
                6, self.receives + step, to["pair"],
            )

        def offer(self, *steps):
            for step in steps:
                theirs = self.part.at[self.order[step], rows_at((1 - core) * 128, 128), :]
                self.pair(theirs, step).start()

        def join(self, step):
            landed = land_pair.at[self.which, step]
            self.pair(landed, step).wait_recv()
            mine = self.part.at[self.order[step], rows_at(core * 128, 128), :]
            mine[...] = (mine[...].astype(F32) + landed[...].astype(F32)).astype(BF)

        def end(self):
            def keep(half, total):
                self.out[pl.ds(half * 64, 64), :] = total.astype(BF)
            self.ring.end(keep)

    loads = [
        pltpu.make_async_copy(up_hbm, up_w.at[z, rows_at(y * 128, 128), :], load_sem.at[0]),
        pltpu.make_async_copy(down_hbm, down_w.at[z, rows_at(y * 128, 128), :], load_sem.at[1]),
        pltpu.make_async_copy(saved_hbm, saved, load_sem.at[2]),
        pltpu.make_async_copy(upstream_hbm, upstream, load_sem.at[3]),
        pltpu.make_async_copy(fresh_hbm, fresh, load_sem.at[4]),
        pltpu.make_async_copy(accum_up_hbm, accum_up, load_sem.at[5]),
        pltpu.make_async_copy(accum_down_hbm, accum_down, load_sem.at[6]),
    ]
    for load in loads:
        load.start()

    barrier = pltpu.get_barrier_semaphore()
    for target in to.values():
        pl.semaphore_signal(barrier, inc=1, device_id=target, device_id_type=MESH)
    pl.semaphore_wait(barrier, len(to))

    up_1, up_2 = gather_1(up_w, 0), (gather_2(up_w, 0, 0), gather_2(up_w, 1, 0))
    down_1, down_2 = gather_1(down_w, 1), (gather_2(down_w, 0, 1), gather_2(down_w, 1, 1))
    grad_up = upstream_t
    down_sum = [GradSum(grad_down, 0, q, accum_down, accum_down_out) for q in range(2)]
    up_sum = [GradSum(grad_up, 1, q, accum_up, accum_up_out) for q in range(2)]
    fresh_sum = TokenSum(fresh, 0, fresh_out)
    saved_sum = TokenSum(saved, 1, saved_grad)

    def turned(rows, out):
        def step(i, carry):
            out[:, :, rows_at(i * 256, 256)] = rows[i].T.reshape(4, 512, 256)
            return carry
        lax.fori_loop(0, 4, step, 0)

    def hidden(q, rows, weight, store, first=0, last=4):
        def step(j, carry):
            i, ab = j // 2, j % 2
            cols = rows_at(ab * 512 + q * 256, 256)
            pre = jnp.dot(
                rows[pl.ds(i * 2, 2)].reshape(512, 2048),
                weight[:, :, cols].reshape(2048, 256), preferred_element_type=F32,
            )
            store(rows_at(i * 512, 512), cols, pre)
            return carry
        lax.fori_loop(first, last, step, 0)

    def keep_saved(at, cols, pre):
        active = jnp.maximum(pre, 0.0)
        saved_active[at, cols] = active.astype(BF)
        saved_hidden[at, cols] = (active * active).astype(BF)

    def keep_fresh(at, cols, pre):
        active = jnp.maximum(pre, 0.0)
        fresh_hidden[at, cols] = (active * active).astype(BF)

    def keep_back(at, cols, hidden_grad):
        active = saved_active[at, cols].astype(F32)
        pre_grad[at, cols] = (2.0 * active * hidden_grad).astype(BF)

    def grad(q, left, right, out, first=0, last=4):
        a, b = GROUPS[q]
        def step(p, carry):
            total = jnp.dot(left[p], right[:, a], preferred_element_type=F32)
            out[p, :, a] = total.astype(BF)
            total = jnp.dot(left[p], right[:, b], preferred_element_type=F32)
            out[p, :, b] = total.astype(BF)
            return carry
        lax.fori_loop(first, last, step, 0)

    def output(q, hidden_rows, weight, part, chunks, first=0, last=4):
        def beside(block):
            if q is None:
                return block[...]
            a, b = GROUPS[q]
            return jnp.concatenate([block[:, a], block[:, b]], axis=1)
        def step(n, carry):
            left = jnp.concatenate(
                [beside(hidden_rows.at[rows_at(c * 256, 256)]) for c in chunks], axis=0
            )
            total = lax.dot_general(
                left, beside(weight.at[n]), (((1,), (1,)), ((), ())), preferred_element_type=F32
            )
            cols = rows_at(n * 512, 512)
            for k, c in enumerate(chunks):
                some = total[k * 256:k * 256 + 256]
                if q == 1:
                    some = part[c, :, cols].astype(F32) + some
                part[c, :, cols] = some.astype(BF)
            return carry
        lax.fori_loop(first, last, step, 0)

    loads[0].wait()
    loads[1].wait()
    up_1.start()
    up_1.rest()
    up_1.mid()
    down_1.start()
    down_1.rest()
    for load in loads[2:]:
        load.wait()
    up_1.end()
    up_2[0].start()
    down_1.mid()
    up_2[0].rest()
    turned(upstream, upstream_t)
    up_2[0].mid()
    up_2[1].start()
    up_2[1].rest()
    down_1.end()
    turned(saved, saved_t)
    up_2[0].end()

    hidden(0, saved, up_w, keep_saved)
    up_2[1].mid()
    down_2[0].start()
    down_2[0].rest()
    hidden(0, fresh, up_w, keep_fresh)
    grad(0, upstream_t, saved_hidden, grad_down)
    up_2[1].end()
    hidden(1, saved, up_w, keep_saved)
    down_2[0].mid()
    down_2[1].start()
    down_2[1].rest()
    grad(1, upstream_t, saved_hidden, grad_down)
    hidden(1, fresh, up_w, keep_fresh)
    down_2[0].end()
    output(0, fresh_hidden, down_w, fresh, fresh_sum.order[:2])
    down_2[1].mid()
    output(0, fresh_hidden, down_w, fresh, fresh_sum.order[2:])
    pl.when(core == 0)(down_sum[0].start)
    down_2[1].end()

    pl.when(core == 1)(down_sum[0].start)
    down_sum[1].start()
    output(1, fresh_hidden, down_w, fresh, fresh_sum.order[:2])
    fresh_sum.offer(0, 1)
    output(1, fresh_hidden, down_w, fresh, fresh_sum.order[2:])
    fresh_sum.offer(2, 3)
    fresh_sum.join(0)
    fresh_sum.ring.start()
    hidden(0, upstream, down_w, keep_back)
    fresh_sum.join(1)
    fresh_sum.join(2)
    fresh_sum.ring.rest()
    fresh_sum.join(3)
    down_sum[0].mid()
    grad(0, saved_t, pre_grad, grad_up)
    up_sum[0].start()
    hidden(1, upstream, down_w, keep_back, 0, 2)
    fresh_sum.ring.mid()
    down_sum[1].mid()
    hidden(1, upstream, down_w, keep_back, 2, 4)
    grad(1, saved_t, pre_grad, grad_up)
    up_sum[1].start()
    output(None, pre_grad, up_w, saved, saved_sum.order[:2])
    saved_sum.offer(0, 1)
    output(None, pre_grad, up_w, saved, saved_sum.order[2:], 0, 2)
    saved_sum.join(0)
    saved_sum.ring.start()
    saved_sum.join(1)
    up_sum[0].mid()
    output(None, pre_grad, up_w, saved, saved_sum.order[2:], 2, 4)
    saved_sum.offer(2, 3)
    down_sum[0].turn()
    saved_sum.join(2)
    saved_sum.ring.rest()
    saved_sum.join(3)
    fresh_sum.end()
    up_sum[1].mid()
    down_sum[1].turn()
    saved_sum.ring.mid()
    down_sum[0].mid_2()
    up_sum[0].turn()
    up_sum[1].turn()
    down_sum[1].mid_2()
    up_sum[0].mid_2()
    up_sum[1].mid_2()
    down_sum[0].end()
    down_sum[1].end()
    up_sum[0].end()
    saved_sum.end()
    up_sum[1].end()
    for index, bulk in enumerate(bulks):
        message(bulk, bulk, index, 0, to["pair"]).wait_send()


def settle(*refs):
    held, out, sems = refs[:4], refs[4:8], refs[8]
    copies = [pltpu.make_async_copy(h, o, sems.at[i]) for i, (h, o) in enumerate(zip(held, out))]
    for copy in copies:
        copy.start()
    for copy in copies:
        copy.wait()


def body(fresh_rows, saved_rows, upstream_grad, proj_up, proj_down, accum_up, accum_down):
    anywhere = pl.BlockSpec(memory_space=pl.ANY)
    inside = pl.BlockSpec(memory_space=pltpu.VMEM)
    shape = jax.ShapeDtypeStruct
    results = pl.pallas_call(
        kernel,
        out_shape=(
            pltpu.VMEM((128, 2048), BF), pltpu.VMEM((128, 2048), BF),
            pltpu.VMEM((128, 1024), F32), pltpu.VMEM((128, 1024), F32),
        ),
        in_specs=[anywhere] * 7,
        out_specs=(inside,) * 4,
        scratch_shapes=[
            pltpu.VMEM((4, 256, 2048), BF),
            pltpu.VMEM((4, 256, 2048), BF),
            pltpu.VMEM((4, 256, 2048), BF),
            pltpu.VMEM((4, 512, 1024), BF),
            pltpu.VMEM((4, 512, 1024), BF),
            pltpu.VMEM((128, 1024), F32),
            pltpu.VMEM((128, 1024), F32),
            pltpu.VMEM((4, 512, 1024), BF),
            pltpu.VMEM((4, 512, 1024), BF),
            pltpu.VMEM((1024, 1024), BF),
            pltpu.VMEM((1024, 1024), BF),
            pltpu.VMEM((1024, 1024), BF),
            pltpu.VMEM((1024, 1024), BF),
            pltpu.VMEM((4, 512, 1024), BF),
            pltpu.VMEM((2, 2, 6, 256, 256), BF),
            pltpu.VMEM((2, 2, 6, 2, 128, 256), BF),
            pltpu.VMEM((2, 2, 2, 6, 64, 256), BF),
            pltpu.VMEM((2, 4, 128, 2048), BF),
            pltpu.VMEM((2, 6, 64, 2048), BF),
            pltpu.SemaphoreType.DMA((7,)),
            pltpu.SemaphoreType.DMA((N_RINGS * 3 + 8,)),
            pltpu.SemaphoreType.DMA((7,)),
        ],
        compiler_params=pltpu.CompilerParams(
            collective_id=0, has_side_effects=True, vmem_limit_bytes=62914560
        ),
        cost_estimate=pl.CostEstimate(
            flops=30064771072, bytes_accessed=32 * 1024 * 1024, transcendentals=0
        ),
    )(
        fresh_rows.reshape(4, 256, 2048), saved_rows.reshape(4, 256, 2048),
        upstream_grad.reshape(4, 256, 2048),
        proj_up, proj_down, accum_up, accum_down,
    )
    return pl.pallas_call(
        settle,
        out_shape=tuple(shape(r.shape, r.dtype) for r in results),
        in_specs=[inside] * 4,
        out_specs=(anywhere,) * 4,
        scratch_shapes=[pltpu.SemaphoreType.DMA((4,))],
    )(*[pltpu.with_memory_space_constraint(r, pltpu.VMEM) for r in results])


def solution(mesh):
    in_specs = (
        P("fs", None),
        P("fs", None),
        P("fs", None),
        P("fs", "tp"),
        P("fs", "tp"),
        P("fs", "tp"),
        P("fs", "tp"),
    )
    out_specs = (P(("fs", "tp"), None), P(("fs", "tp"), None), P("fs", "tp"), P("fs", "tp"))
    return jax.shard_map(body, mesh=mesh, in_specs=in_specs, out_specs=out_specs, check_vma=False)
```

```python
import jax
import jax.numpy as jnp
from jax import lax
from jax.experimental import pallas as pl
from jax.experimental.pallas import tpu as pltpu
from jax.sharding import PartitionSpec as P

MESH = pl.DeviceIdType.MESH
BF = jnp.bfloat16
F32 = jnp.float32
COLS = (slice(0, 512), slice(512, 1024))
GROUPS = tuple((slice(q, q + 256), slice(q + 512, q + 768)) for q in (0, 256))
N_RINGS = 14 + 16 + 2


def rows_at(start, size):
    return pl.ds(pl.multiple_of(start, size), size)


def kernel(
    fresh_hbm, saved_hbm, upstream_hbm, up_hbm, down_hbm, accum_up_hbm, accum_down_hbm,
    fresh_out, saved_grad, accum_up_out, accum_down_out,
    fresh, saved, upstream, up_w, down_w, accum_up, accum_down,
    saved_t, upstream_t, fresh_hidden, saved_active, saved_hidden, pre_grad, grad_down,
    land_z, land_y, land_2, land_pair, land_x,
    send_sem, recv_sem, load_sem,
):
    fs, tp = lax.axis_index("fs"), lax.axis_index("tp")
    z, y, x, core = fs // 4, fs % 4, tp // 2, tp % 2

    def nxt(p, by):
        return lax.rem(p + by, 4)

    to = {
        ("y", 1): (z * 4 + nxt(y, 1), tp),
        ("y", -1): (z * 4 + nxt(y, 3), tp),
        ("z", 1): (nxt(z, 1) * 4 + y, tp),
        ("z", -1): (nxt(z, 3) * 4 + y, tp),
        ("x", 1): (fs, nxt(x, 1) * 2 + core),
        ("x", -1): (fs, nxt(x, 3) * 2 + core),
        "pair": (fs, x * 2 + 1 - core),
    }
    place = {"y": y, "z": z, "x": x}
    used = [0]
    part_of = (slice(None), pl.ds(0, 480))
    bulks = (up_w.at[part_of], down_w.at[part_of], land_z, land_y, land_2, land_x, land_pair)

    def reserve(count):
        used[0] += count
        return used[0] - count

    def message(src, dst, sends, receives, target):
        return pltpu.make_async_remote_copy(
            src_ref=src,
            dst_ref=dst,
            send_sem=send_sem.at[sends],
            recv_sem=recv_sem.at[receives],
            device_id=target,
            device_id_type=MESH,
        )

    class Ring:
        def __init__(self, axis, pool):
            self.plus, self.minus = to[(axis, 1)], to[(axis, -1)]
            p = place[axis]
            self.here, self.after, self.across, self.before = p, nxt(p, 1), nxt(p, 2), nxt(p, 3)
            self.out, self.into = pool, reserve(3)

        def push(self, src, dst, slot, target):
            message(src, dst, self.out, self.into + slot, target).start()

        def got(self, dst, slot):
            message(dst, dst, self.out, self.into + slot, self.plus).wait_recv()

    class Gather(Ring):
        def __init__(self, axis, block, two, pool):
            super().__init__(axis, pool)
            self.block, self.two = block, two

        def go(self, half, slot, owner, target):
            part = self.block(owner, half)
            self.push(part, part, slot, target)

        def start(self):
            self.go(0, 0, self.here, self.plus)
            self.go(1, 1, self.here, self.minus)

        def rest(self):
            self.go(1, 2, self.here, self.plus)
            self.go(0, 2, self.here, self.minus)

        def mid(self):
            self.got(self.block(self.before, 0), 0)
            self.go(0, 2, self.before, self.plus)
            self.got(self.block(self.after, 1), 1)
            self.go(1, 2, self.after, self.minus)

        def end(self):
            self.got(self.two, 2)

    class Scatter(Ring):
        def __init__(self, axis, block, land, pool):
            super().__init__(axis, pool)
            self.block, self.land = block, land

        def go(self, half, slot, index, owner, target):
            self.push(self.block(owner, half), self.land.at[index], slot, target)

        def add(self, owner, half, index):
            mine = self.block(owner, half)
            mine[...] = (mine[...].astype(F32) + self.land[index].astype(F32)).astype(BF)

        def start(self):
            self.go(0, 0, 0, self.across, self.plus)
            self.go(1, 1, 1, self.across, self.minus)

        def rest(self):
            self.go(1, 2, 2, self.after, self.plus)
            self.go(0, 2, 3, self.before, self.minus)

        def mid(self):
            self.got(self.land.at[0], 0)
            self.add(self.after, 0, 0)
            self.go(0, 2, 4, self.after, self.plus)
            self.got(self.land.at[1], 1)
            self.add(self.before, 1, 1)
            self.go(1, 2, 5, self.before, self.minus)

        def end(self, store):
            self.got(self.land.at[pl.ds(2, 4)], 2)
            for half, parts in ((0, (3, 4)), (1, (2, 5))):
                total = self.block(self.here, half)[...].astype(F32)
                for index in parts:
                    total = total + self.land[index].astype(F32)
                store(half, total)

    class Both:
        def __init__(self, *rings):
            self.rings = rings

        def __getattr__(self, step):
            def run():
                for ring in self.rings:
                    getattr(ring, step)()
            return run

    def gather_1(w, cols, pool):
        a, b = cols
        return Both(
            Gather(
                "y", lambda p, h: w.at[z, rows_at(p * 128 + h * 64, 64), a],
                w.at[0, pl.ds(0, 256), a], pool,
            ),
            Gather(
                "z", lambda p, h: w.at[p, rows_at(y * 128 + h * 64, 64), b],
                w.at[0, pl.ds(0, 256), b], pool,
            ),
        )

    def gather_2(w, q, pool):
        a, b = GROUPS[q]
        return Both(
            Gather(
                "z", lambda p, h: w.at[p, pl.ds(h * 256, 256), a],
                w.at[pl.ds(0, 2), :, a], pool,
            ),
            Gather(
                "y", lambda p, h: w.at[pl.ds(h * 2, 2), rows_at(p * 128, 128), b],
                w.at[:, pl.ds(0, 256), b], pool,
            ),
        )

    class GradSum:
        def __init__(self, grad, which, q, accum, out):
            a, b = GROUPS[q]
            self.q, self.accum, self.out = q, accum, out
            self.one = (
                Scatter(
                    "z", lambda p, h: grad.at[p, pl.ds(h * 256, 256), a],
                    land_z.at[which, q], 2,
                ),
                Scatter(
                    "y", lambda p, h: grad.at[pl.ds(h * 2, 2), rows_at(p * 128, 128), b],
                    land_y.at[which, q], 3,
                ),
            )
            self.two = (
                Scatter(
                    "y", lambda p, h: grad.at[z, rows_at(p * 128 + h * 64, 64), a],
                    land_2.at[which, q, 0], 4,
                ),
                Scatter(
                    "z", lambda p, h: grad.at[p, rows_at(y * 128 + h * 64, 64), b],
                    land_2.at[which, q, 1], 4,
                ),
            )

        def start(self):
            for ring in self.one:
                ring.start()
            for ring in self.one:
                ring.rest()

        def mid(self):
            for ring in self.one:
                ring.mid()

        def turn(self):
            for ring, after in zip(self.one, self.two):
                def keep(half, total, ring=ring):
                    ring.block(ring.here, half)[...] = total.astype(BF)
                ring.end(keep)
                after.start()
                after.rest()

        def mid_2(self):
            for ring in self.two:
                ring.mid()

        def end(self):
            for ring, cols in zip(self.two, GROUPS[self.q]):
                def keep(half, total, cols=cols):
                    rows = pl.ds(half * 64, 64)
                    self.out[rows, cols] = self.accum[rows, cols] + 0.0078125 * total
                ring.end(keep)

    class TokenSum:
        def __init__(self, part, which, out):
            self.part, self.which, self.out = part, which, out
            self.receives = reserve(4)
            self.order = (nxt(x, 2), nxt(x, 1), nxt(x, 3), x)
            self.ring = Scatter(
                "x", lambda p, h: part.at[p, rows_at(core * 128 + h * 64, 64), :],
                land_x.at[which], 5,
            )

        def pair(self, src, step):
            return message(
                src, land_pair.at[self.which, step],
                6, self.receives + step, to["pair"],
            )

        def offer(self, *steps):
            for step in steps:
                theirs = self.part.at[self.order[step], rows_at((1 - core) * 128, 128), :]
                self.pair(theirs, step).start()

        def join(self, step):
            landed = land_pair.at[self.which, step]
            self.pair(landed, step).wait_recv()
            mine = self.part.at[self.order[step], rows_at(core * 128, 128), :]
            mine[...] = (mine[...].astype(F32) + landed[...].astype(F32)).astype(BF)

        def end(self):
            def keep(half, total):
                self.out[pl.ds(half * 64, 64), :] = total.astype(BF)
            self.ring.end(keep)

    loads = [
        pltpu.make_async_copy(up_hbm, up_w.at[z, rows_at(y * 128, 128), :], load_sem.at[0]),
        pltpu.make_async_copy(down_hbm, down_w.at[z, rows_at(y * 128, 128), :], load_sem.at[1]),
        pltpu.make_async_copy(saved_hbm, saved, load_sem.at[2]),
        pltpu.make_async_copy(upstream_hbm, upstream, load_sem.at[3]),
        pltpu.make_async_copy(fresh_hbm, fresh, load_sem.at[4]),
        pltpu.make_async_copy(accum_up_hbm, accum_up, load_sem.at[5]),
        pltpu.make_async_copy(accum_down_hbm, accum_down, load_sem.at[6]),
    ]
    for load in loads:
        load.start()

    barrier = pltpu.get_barrier_semaphore()
    for target in to.values():
        pl.semaphore_signal(barrier, inc=1, device_id=target, device_id_type=MESH)
    pl.semaphore_wait(barrier, len(to))

    up_1 = [gather_1(up_w, cols, 0) for cols in GROUPS]
    up_2, down_1 = (gather_2(up_w, 0, 0), gather_2(up_w, 1, 0)), gather_1(down_w, COLS, 1)
    down_2 = (gather_2(down_w, 0, 1), gather_2(down_w, 1, 1))
    grad_up = upstream_t
    down_sum = [GradSum(grad_down, 0, q, accum_down, accum_down_out) for q in range(2)]
    up_sum = [GradSum(grad_up, 1, q, accum_up, accum_up_out) for q in range(2)]
    fresh_sum = TokenSum(fresh, 0, fresh_out)
    saved_sum = TokenSum(saved, 1, saved_grad)

    def turned(rows, out):
        def step(i, carry):
            out[:, :, rows_at(i * 256, 256)] = rows[i].T.reshape(4, 512, 256)
            return carry
        lax.fori_loop(0, 4, step, 0)

    def hidden(q, rows, weight, store, first=0, last=4):
        def step(j, carry):
            i, ab = j // 2, j % 2
            cols = rows_at(ab * 512 + q * 256, 256)
            pre = jnp.dot(
                rows[pl.ds(i * 2, 2)].reshape(512, 2048),
                weight[:, :, cols].reshape(2048, 256), preferred_element_type=F32,
            )
            store(rows_at(i * 512, 512), cols, pre)
            return carry
        lax.fori_loop(first, last, step, 0)

    def keep_saved(at, cols, pre):
        active = jnp.maximum(pre, 0.0)
        saved_active[at, cols] = active.astype(BF)
        saved_hidden[at, cols] = (active * active).astype(BF)

    def keep_fresh(at, cols, pre):
        active = jnp.maximum(pre, 0.0)
        fresh_hidden[at, cols] = (active * active).astype(BF)

    def keep_back(at, cols, hidden_grad):
        active = saved_active[at, cols].astype(F32)
        pre_grad[at, cols] = (2.0 * active * hidden_grad).astype(BF)

    def grad(q, left, right, out, first=0, last=4):
        a, b = GROUPS[q]
        def step(p, carry):
            total = jnp.dot(left[p], right[:, a], preferred_element_type=F32)
            out[p, :, a] = total.astype(BF)
            total = jnp.dot(left[p], right[:, b], preferred_element_type=F32)
            out[p, :, b] = total.astype(BF)
            return carry
        lax.fori_loop(first, last, step, 0)

    def output(q, hidden_rows, weight, part, chunks, first=0, last=4):
        def beside(block):
            if q is None:
                return block[...]
            a, b = GROUPS[q]
            return jnp.concatenate([block[:, a], block[:, b]], axis=1)
        def step(n, carry):
            left = jnp.concatenate(
                [beside(hidden_rows.at[rows_at(c * 256, 256)]) for c in chunks], axis=0
            )
            total = lax.dot_general(
                left, beside(weight.at[n]), (((1,), (1,)), ((), ())), preferred_element_type=F32
            )
            cols = rows_at(n * 512, 512)
            for k, c in enumerate(chunks):
                some = total[k * 256:k * 256 + 256]
                if q == 1:
                    some = part[c, :, cols].astype(F32) + some
                part[c, :, cols] = some.astype(BF)
            return carry
        lax.fori_loop(first, last, step, 0)

    loads[0].wait()
    loads[1].wait()
    for ring in up_1:
        ring.start()
        ring.rest()
    up_1[0].mid()
    down_1.start()
    down_1.rest()
    up_1[1].mid()
    for load in loads[2:]:
        load.wait()
    up_1[0].end()
    up_2[0].start()
    down_1.mid()
    up_2[0].rest()
    turned(upstream, upstream_t)
    up_2[0].mid()
    up_1[1].end()
    up_2[1].start()
    up_2[1].rest()
    down_1.end()
    turned(saved, saved_t)
    up_2[0].end()

    hidden(0, saved, up_w, keep_saved)
    up_2[1].mid()
    down_2[0].start()
    down_2[0].rest()
    hidden(0, fresh, up_w, keep_fresh)
    grad(0, upstream_t, saved_hidden, grad_down)
    up_2[1].end()
    hidden(1, saved, up_w, keep_saved)
    down_2[0].mid()
    down_2[1].start()
    down_2[1].rest()
    grad(1, upstream_t, saved_hidden, grad_down)
    hidden(1, fresh, up_w, keep_fresh)
    down_2[0].end()
    output(0, fresh_hidden, down_w, fresh, fresh_sum.order[:2])
    down_2[1].mid()
    output(0, fresh_hidden, down_w, fresh, fresh_sum.order[2:])
    pl.when(core == 0)(down_sum[0].start)
    down_2[1].end()
    pl.when(core == 1)(down_sum[0].start)

    output(1, fresh_hidden, down_w, fresh, fresh_sum.order[:1])
    fresh_sum.offer(0)
    output(1, fresh_hidden, down_w, fresh, fresh_sum.order[1:2])
    fresh_sum.offer(1)
    down_sum[1].start()
    output(1, fresh_hidden, down_w, fresh, fresh_sum.order[2:], 0, 2)
    fresh_sum.join(0)
    fresh_sum.ring.start()
    output(1, fresh_hidden, down_w, fresh, fresh_sum.order[2:], 2, 4)
    fresh_sum.offer(2, 3)
    hidden(0, upstream, down_w, keep_back)
    fresh_sum.join(1)
    fresh_sum.join(2)
    fresh_sum.ring.rest()
    fresh_sum.join(3)
    down_sum[0].mid()
    grad(0, saved_t, pre_grad, grad_up)
    up_sum[0].start()
    hidden(1, upstream, down_w, keep_back, 0, 2)
    fresh_sum.ring.mid()
    down_sum[1].mid()
    hidden(1, upstream, down_w, keep_back, 2, 4)
    grad(1, saved_t, pre_grad, grad_up)
    up_sum[1].start()
    output(None, pre_grad, up_w, saved, saved_sum.order[:2])
    saved_sum.offer(0, 1)
    output(None, pre_grad, up_w, saved, saved_sum.order[2:], 0, 2)
    saved_sum.join(0)
    saved_sum.ring.start()
    saved_sum.join(1)
    up_sum[0].mid()
    output(None, pre_grad, up_w, saved, saved_sum.order[2:], 2, 4)
    saved_sum.offer(2, 3)
    down_sum[0].turn()
    saved_sum.join(2)
    saved_sum.ring.rest()
    saved_sum.join(3)
    fresh_sum.end()
    up_sum[1].mid()
    down_sum[1].turn()
    saved_sum.ring.mid()
    down_sum[0].mid_2()
    up_sum[0].turn()
    up_sum[1].turn()
    down_sum[1].mid_2()
    up_sum[0].mid_2()
    up_sum[1].mid_2()
    down_sum[0].end()
    down_sum[1].end()
    up_sum[0].end()
    saved_sum.end()
    up_sum[1].end()
    for index, bulk in enumerate(bulks):
        message(bulk, bulk, index, 0, to["pair"]).wait_send()


def settle(*refs):
    held, out, sems = refs[:4], refs[4:8], refs[8]
    copies = [pltpu.make_async_copy(h, o, sems.at[i]) for i, (h, o) in enumerate(zip(held, out))]
    for copy in copies:
        copy.start()
    for copy in copies:
        copy.wait()


def body(fresh_rows, saved_rows, upstream_grad, proj_up, proj_down, accum_up, accum_down):
    anywhere = pl.BlockSpec(memory_space=pl.ANY)
    inside = pl.BlockSpec(memory_space=pltpu.VMEM)
    shape = jax.ShapeDtypeStruct
    results = pl.pallas_call(
        kernel,
        out_shape=(
            pltpu.VMEM((128, 2048), BF), pltpu.VMEM((128, 2048), BF),
            pltpu.VMEM((128, 1024), F32), pltpu.VMEM((128, 1024), F32),
        ),
        in_specs=[anywhere] * 7,
        out_specs=(inside,) * 4,
        scratch_shapes=[
            pltpu.VMEM((4, 256, 2048), BF),
            pltpu.VMEM((4, 256, 2048), BF),
            pltpu.VMEM((4, 256, 2048), BF),
            pltpu.VMEM((4, 512, 1024), BF),
            pltpu.VMEM((4, 512, 1024), BF),
            pltpu.VMEM((128, 1024), F32),
            pltpu.VMEM((128, 1024), F32),
            pltpu.VMEM((4, 512, 1024), BF),
            pltpu.VMEM((4, 512, 1024), BF),
            pltpu.VMEM((1024, 1024), BF),
            pltpu.VMEM((1024, 1024), BF),
            pltpu.VMEM((1024, 1024), BF),
            pltpu.VMEM((1024, 1024), BF),
            pltpu.VMEM((4, 512, 1024), BF),
            pltpu.VMEM((2, 2, 6, 256, 256), BF),
            pltpu.VMEM((2, 2, 6, 2, 128, 256), BF),
            pltpu.VMEM((2, 2, 2, 6, 64, 256), BF),
            pltpu.VMEM((2, 4, 128, 2048), BF),
            pltpu.VMEM((2, 6, 64, 2048), BF),
            pltpu.SemaphoreType.DMA((7,)),
            pltpu.SemaphoreType.DMA((N_RINGS * 3 + 8,)),
            pltpu.SemaphoreType.DMA((7,)),
        ],
        compiler_params=pltpu.CompilerParams(
            collective_id=0, has_side_effects=True, vmem_limit_bytes=62914560
        ),
        cost_estimate=pl.CostEstimate(
            flops=30064771072, bytes_accessed=32 * 1024 * 1024, transcendentals=0
        ),
    )(
        fresh_rows.reshape(4, 256, 2048), saved_rows.reshape(4, 256, 2048),
        upstream_grad.reshape(4, 256, 2048),
        proj_up, proj_down, accum_up, accum_down,
    )
    return pl.pallas_call(
        settle,
        out_shape=tuple(shape(r.shape, r.dtype) for r in results),
        in_specs=[inside] * 4,
        out_specs=(anywhere,) * 4,
        scratch_shapes=[pltpu.SemaphoreType.DMA((4,))],
    )(*[pltpu.with_memory_space_constraint(r, pltpu.VMEM) for r in results])


def solution(mesh):
    in_specs = (
        P("fs", None),
        P("fs", None),
        P("fs", None),
        P("fs", "tp"),
        P("fs", "tp"),
        P("fs", "tp"),
        P("fs", "tp"),
    )
    out_specs = (P(("fs", "tp"), None), P(("fs", "tp"), None), P("fs", "tp"), P("fs", "tp"))
    return jax.shard_map(body, mesh=mesh, in_specs=in_specs, out_specs=out_specs, check_vma=False)
```

```python
import jax
import jax.numpy as jnp
from jax import lax
from jax.experimental import pallas as pl
from jax.experimental.pallas import tpu as pltpu
from jax.sharding import PartitionSpec as P

MESH = pl.DeviceIdType.MESH
BF = jnp.bfloat16
F32 = jnp.float32
COLS = (slice(0, 512), slice(512, 1024))
GROUPS = tuple((slice(q, q + 256), slice(q + 512, q + 768)) for q in (0, 256))
N_RINGS = 14 + 16 + 2


def rows_at(start, size):
    return pl.ds(pl.multiple_of(start, size), size)


def kernel(
    fresh_hbm, saved_hbm, upstream_hbm, up_hbm, down_hbm, accum_up_hbm, accum_down_hbm,
    fresh_out, saved_grad, accum_up_out, accum_down_out,
    fresh, saved, upstream, up_w, down_w, accum_up, accum_down,
    saved_t, upstream_t, fresh_hidden, saved_active, saved_hidden, pre_grad, grad_down,
    land_z, land_y, land_2, land_pair, land_x,
    send_sem, recv_sem, load_sem,
):
    fs, tp = lax.axis_index("fs"), lax.axis_index("tp")
    z, y, x, core = fs // 4, fs % 4, tp // 2, tp % 2

    def nxt(p, by):
        return lax.rem(p + by, 4)

    to = {
        ("y", 1): (z * 4 + nxt(y, 1), tp),
        ("y", -1): (z * 4 + nxt(y, 3), tp),
        ("z", 1): (nxt(z, 1) * 4 + y, tp),
        ("z", -1): (nxt(z, 3) * 4 + y, tp),
        ("x", 1): (fs, nxt(x, 1) * 2 + core),
        ("x", -1): (fs, nxt(x, 3) * 2 + core),
        "pair": (fs, x * 2 + 1 - core),
    }
    place = {"y": y, "z": z, "x": x}
    used = [0]
    part_of = (slice(None), pl.ds(0, 480))
    bulks = (up_w.at[part_of], down_w.at[part_of], land_z, land_y, land_2, land_x, land_pair)

    def reserve(count):
        used[0] += count
        return used[0] - count

    def message(src, dst, sends, receives, target):
        return pltpu.make_async_remote_copy(
            src_ref=src,
            dst_ref=dst,
            send_sem=send_sem.at[sends],
            recv_sem=recv_sem.at[receives],
            device_id=target,
            device_id_type=MESH,
        )

    class Ring:
        def __init__(self, axis, pool):
            self.plus, self.minus = to[(axis, 1)], to[(axis, -1)]
            p = place[axis]
            self.here, self.after, self.across, self.before = p, nxt(p, 1), nxt(p, 2), nxt(p, 3)
            self.out, self.into = pool, reserve(3)

        def push(self, src, dst, slot, target):
            message(src, dst, self.out, self.into + slot, target).start()

        def got(self, dst, slot):
            message(dst, dst, self.out, self.into + slot, self.plus).wait_recv()

    class Gather(Ring):
        def __init__(self, axis, block, two, pool):
            super().__init__(axis, pool)
            self.block, self.two = block, two

        def go(self, half, slot, owner, target):
            part = self.block(owner, half)
            self.push(part, part, slot, target)

        def start(self):
            self.go(0, 0, self.here, self.plus)
            self.go(1, 1, self.here, self.minus)

        def rest(self):
            self.go(1, 2, self.here, self.plus)
            self.go(0, 2, self.here, self.minus)

        def mid(self):
            self.got(self.block(self.before, 0), 0)
            self.go(0, 2, self.before, self.plus)
            self.got(self.block(self.after, 1), 1)
            self.go(1, 2, self.after, self.minus)

        def end(self):
            self.got(self.two, 2)

    class Scatter(Ring):
        def __init__(self, axis, block, land, pool):
            super().__init__(axis, pool)
            self.block, self.land = block, land

        def go(self, half, slot, index, owner, target):
            self.push(self.block(owner, half), self.land.at[index], slot, target)

        def add(self, owner, half, index):
            mine = self.block(owner, half)
            mine[...] = (mine[...].astype(F32) + self.land[index].astype(F32)).astype(BF)

        def start(self):
            self.go(0, 0, 0, self.across, self.plus)
            self.go(1, 1, 1, self.across, self.minus)

        def rest(self):
            self.go(1, 2, 2, self.after, self.plus)
            self.go(0, 2, 3, self.before, self.minus)

        def mid(self):
            self.got(self.land.at[0], 0)
            self.add(self.after, 0, 0)
            self.go(0, 2, 4, self.after, self.plus)
            self.got(self.land.at[1], 1)
            self.add(self.before, 1, 1)
            self.go(1, 2, 5, self.before, self.minus)

        def end(self, store):
            self.got(self.land.at[pl.ds(2, 4)], 2)
            for half, parts in ((0, (3, 4)), (1, (2, 5))):
                total = self.block(self.here, half)[...].astype(F32)
                for index in parts:
                    total = total + self.land[index].astype(F32)
                store(half, total)

    class Both:
        def __init__(self, *rings):
            self.rings = rings

        def __getattr__(self, step):
            def run():
                for ring in self.rings:
                    getattr(ring, step)()
            return run

    def gather_1(w, cols, pool):
        a, b = cols
        return Both(
            Gather(
                "y", lambda p, h: w.at[z, rows_at(p * 128 + h * 64, 64), a],
                w.at[0, pl.ds(0, 256), a], pool,
            ),
            Gather(
                "z", lambda p, h: w.at[p, rows_at(y * 128 + h * 64, 64), b],
                w.at[0, pl.ds(0, 256), b], pool,
            ),
        )

    def gather_2(w, q, pool):
        a, b = GROUPS[q]
        return Both(
            Gather(
                "z", lambda p, h: w.at[p, pl.ds(h * 256, 256), a],
                w.at[pl.ds(0, 2), :, a], pool,
            ),
            Gather(
                "y", lambda p, h: w.at[pl.ds(h * 2, 2), rows_at(p * 128, 128), b],
                w.at[:, pl.ds(0, 256), b], pool,
            ),
        )

    class GradSum:
        def __init__(self, grad, which, q, accum, out):
            a, b = GROUPS[q]
            self.q, self.accum, self.out = q, accum, out
            self.one = (
                Scatter(
                    "z", lambda p, h: grad.at[p, pl.ds(h * 256, 256), a],
                    land_z.at[which, q], 2,
                ),
                Scatter(
                    "y", lambda p, h: grad.at[pl.ds(h * 2, 2), rows_at(p * 128, 128), b],
                    land_y.at[which, q], 3,
                ),
            )
            self.two = (
                Scatter(
                    "y", lambda p, h: grad.at[z, rows_at(p * 128 + h * 64, 64), a],
                    land_2.at[which, q, 0], 4,
                ),
                Scatter(
                    "z", lambda p, h: grad.at[p, rows_at(y * 128 + h * 64, 64), b],
                    land_2.at[which, q, 1], 4,
                ),
            )

        def start(self):
            for ring in self.one:
                ring.start()
            for ring in self.one:
                ring.rest()

        def mid(self):
            for ring in self.one:
                ring.mid()

        def turn(self):
            for ring, after in zip(self.one, self.two):
                def keep(half, total, ring=ring):
                    ring.block(ring.here, half)[...] = total.astype(BF)
                ring.end(keep)
                after.start()
                after.rest()

        def mid_2(self):
            for ring in self.two:
                ring.mid()

        def end(self):
            for ring, cols in zip(self.two, GROUPS[self.q]):
                def keep(half, total, cols=cols):
                    rows = pl.ds(half * 64, 64)
                    self.out[rows, cols] = self.accum[rows, cols] + 0.0078125 * total
                ring.end(keep)

    class TokenSum:
        def __init__(self, part, which, out):
            self.part, self.which, self.out = part, which, out
            self.receives = reserve(4)
            self.order = (nxt(x, 2), nxt(x, 1), nxt(x, 3), x)
            self.ring = Scatter(
                "x", lambda p, h: part.at[p, rows_at(core * 128 + h * 64, 64), :],
                land_x.at[which], 5,
            )

        def pair(self, src, step):
            return message(
                src, land_pair.at[self.which, step],
                6, self.receives + step, to["pair"],
            )

        def offer(self, *steps):
            for step in steps:
                theirs = self.part.at[self.order[step], rows_at((1 - core) * 128, 128), :]
                self.pair(theirs, step).start()

        def join(self, step):
            landed = land_pair.at[self.which, step]
            self.pair(landed, step).wait_recv()
            mine = self.part.at[self.order[step], rows_at(core * 128, 128), :]
            mine[...] = (mine[...].astype(F32) + landed[...].astype(F32)).astype(BF)

        def end(self):
            def keep(half, total):
                self.out[pl.ds(half * 64, 64), :] = total.astype(BF)
            self.ring.end(keep)

    loads = [
        pltpu.make_async_copy(up_hbm, up_w.at[z, rows_at(y * 128, 128), :], load_sem.at[0]),
        pltpu.make_async_copy(down_hbm, down_w.at[z, rows_at(y * 128, 128), :], load_sem.at[1]),
        pltpu.make_async_copy(saved_hbm, saved, load_sem.at[2]),
        pltpu.make_async_copy(upstream_hbm, upstream, load_sem.at[3]),
        pltpu.make_async_copy(fresh_hbm, fresh, load_sem.at[4]),
        pltpu.make_async_copy(accum_up_hbm, accum_up, load_sem.at[5]),
        pltpu.make_async_copy(accum_down_hbm, accum_down, load_sem.at[6]),
    ]
    for load in loads:
        load.start()

    barrier = pltpu.get_barrier_semaphore()
    for target in to.values():
        pl.semaphore_signal(barrier, inc=1, device_id=target, device_id_type=MESH)
    pl.semaphore_wait(barrier, len(to))

    up_1 = [gather_1(up_w, cols, 0) for cols in GROUPS]
    up_2, down_1 = (gather_2(up_w, 0, 0), gather_2(up_w, 1, 0)), gather_1(down_w, COLS, 1)
    down_2 = (gather_2(down_w, 0, 1), gather_2(down_w, 1, 1))
    grad_up = upstream_t
    down_sum = [GradSum(grad_down, 0, q, accum_down, accum_down_out) for q in range(2)]
    up_sum = [GradSum(grad_up, 1, q, accum_up, accum_up_out) for q in range(2)]
    fresh_sum = TokenSum(fresh, 0, fresh_out)
    saved_sum = TokenSum(saved, 1, saved_grad)

    def turned(rows, out):
        def step(i, carry):
            out[:, :, rows_at(i * 256, 256)] = rows[i].T.reshape(4, 512, 256)
            return carry
        lax.fori_loop(0, 4, step, 0)

    def hidden(q, rows, weight, store, first=0, last=4):
        def step(j, carry):
            i, ab = j // 2, j % 2
            cols = rows_at(ab * 512 + q * 256, 256)
            pre = jnp.dot(
                rows[pl.ds(i * 2, 2)].reshape(512, 2048),
                weight[:, :, cols].reshape(2048, 256), preferred_element_type=F32,
            )
            store(rows_at(i * 512, 512), cols, pre)
            return carry
        lax.fori_loop(first, last, step, 0)

    def keep_saved(at, cols, pre):
        active = jnp.maximum(pre, 0.0)
        saved_active[at, cols] = active.astype(BF)
        saved_hidden[at, cols] = (active * active).astype(BF)

    def keep_fresh(at, cols, pre):
        active = jnp.maximum(pre, 0.0)
        fresh_hidden[at, cols] = (active * active).astype(BF)

    def keep_back(at, cols, hidden_grad):
        active = saved_active[at, cols].astype(F32)
        pre_grad[at, cols] = (2.0 * active * hidden_grad).astype(BF)

    def grad(q, left, right, out, first=0, last=4):
        a, b = GROUPS[q]
        def step(p, carry):
            total = jnp.dot(left[p], right[:, a], preferred_element_type=F32)
            out[p, :, a] = total.astype(BF)
            total = jnp.dot(left[p], right[:, b], preferred_element_type=F32)
            out[p, :, b] = total.astype(BF)
            return carry
        lax.fori_loop(first, last, step, 0)

    def output(q, hidden_rows, weight, part, chunks, first=0, last=4):
        def beside(block):
            if q is None:
                return block[...]
            a, b = GROUPS[q]
            return jnp.concatenate([block[:, a], block[:, b]], axis=1)
        def step(n, carry):
            left = jnp.concatenate(
                [beside(hidden_rows.at[rows_at(c * 256, 256)]) for c in chunks], axis=0
            )
            total = lax.dot_general(
                left, beside(weight.at[n]), (((1,), (1,)), ((), ())), preferred_element_type=F32
            )
            cols = rows_at(n * 512, 512)
            for k, c in enumerate(chunks):
                some = total[k * 256:k * 256 + 256]
                if q == 1:
                    some = part[c, :, cols].astype(F32) + some
                part[c, :, cols] = some.astype(BF)
            return carry
        lax.fori_loop(first, last, step, 0)

    loads[0].wait()
    loads[1].wait()
    for ring in up_1:
        ring.start()
        ring.rest()
    up_1[0].mid()
    down_1.start()
    down_1.rest()
    up_1[1].mid()
    for load in loads[2:]:
        load.wait()
    up_1[0].end()
    up_2[0].start()
    down_1.mid()
    up_2[0].rest()
    turned(upstream, upstream_t)
    up_2[0].mid()
    up_1[1].end()
    up_2[1].start()
    up_2[1].rest()
    down_1.end()
    turned(saved, saved_t)
    up_2[0].end()

    hidden(0, saved, up_w, keep_saved)
    up_2[1].mid()
    down_2[0].start()
    down_2[0].rest()
    hidden(0, fresh, up_w, keep_fresh)
    grad(0, upstream_t, saved_hidden, grad_down)
    up_2[1].end()
    hidden(1, saved, up_w, keep_saved)
    down_2[0].mid()
    down_2[1].start()
    down_2[1].rest()
    grad(1, upstream_t, saved_hidden, grad_down)
    hidden(1, fresh, up_w, keep_fresh)
    down_2[0].end()
    output(0, fresh_hidden, down_w, fresh, fresh_sum.order[:2])
    down_2[1].mid()
    output(0, fresh_hidden, down_w, fresh, fresh_sum.order[2:])
    pl.when(core == 0)(down_sum[0].start)
    down_2[1].end()

    output(1, fresh_hidden, down_w, fresh, fresh_sum.order[:1])
    fresh_sum.offer(0)
    pl.when(core == 1)(down_sum[0].start)
    down_sum[1].start()
    output(1, fresh_hidden, down_w, fresh, fresh_sum.order[1:2])
    fresh_sum.offer(1)
    output(1, fresh_hidden, down_w, fresh, fresh_sum.order[2:], 0, 2)
    fresh_sum.join(0)
    fresh_sum.ring.start()
    output(1, fresh_hidden, down_w, fresh, fresh_sum.order[2:], 2, 4)
    fresh_sum.offer(2, 3)
    hidden(0, upstream, down_w, keep_back)
    fresh_sum.join(1)
    fresh_sum.join(2)
    fresh_sum.ring.rest()
    fresh_sum.join(3)
    down_sum[0].mid()
    grad(0, saved_t, pre_grad, grad_up)
    up_sum[0].start()
    hidden(1, upstream, down_w, keep_back, 0, 2)
    fresh_sum.ring.mid()
    down_sum[1].mid()
    hidden(1, upstream, down_w, keep_back, 2, 4)
    grad(1, saved_t, pre_grad, grad_up)
    up_sum[1].start()
    output(None, pre_grad, up_w, saved, saved_sum.order[:1])
    saved_sum.offer(0)
    output(None, pre_grad, up_w, saved, saved_sum.order[1:2])
    saved_sum.offer(1)
    saved_sum.join(0)
    saved_sum.ring.start()
    up_sum[0].mid()
    output(None, pre_grad, up_w, saved, saved_sum.order[2:])
    saved_sum.offer(2, 3)
    saved_sum.join(1)
    down_sum[0].turn()
    saved_sum.join(2)
    saved_sum.ring.rest()
    saved_sum.join(3)
    fresh_sum.end()
    up_sum[1].mid()
    down_sum[1].turn()
    saved_sum.ring.mid()
    down_sum[0].mid_2()
    up_sum[0].turn()
    up_sum[1].turn()
    down_sum[1].mid_2()
    up_sum[0].mid_2()
    up_sum[1].mid_2()
    down_sum[0].end()
    down_sum[1].end()
    up_sum[0].end()
    saved_sum.end()
    up_sum[1].end()
    for index, bulk in enumerate(bulks):
        message(bulk, bulk, index, 0, to["pair"]).wait_send()


def settle(*refs):
    held, out, sems = refs[:4], refs[4:8], refs[8]
    copies = [pltpu.make_async_copy(h, o, sems.at[i]) for i, (h, o) in enumerate(zip(held, out))]
    for copy in copies:
        copy.start()
    for copy in copies:
        copy.wait()


def body(fresh_rows, saved_rows, upstream_grad, proj_up, proj_down, accum_up, accum_down):
    anywhere = pl.BlockSpec(memory_space=pl.ANY)
    inside = pl.BlockSpec(memory_space=pltpu.VMEM)
    shape = jax.ShapeDtypeStruct
    results = pl.pallas_call(
        kernel,
        out_shape=(
            pltpu.VMEM((128, 2048), BF), pltpu.VMEM((128, 2048), BF),
            pltpu.VMEM((128, 1024), F32), pltpu.VMEM((128, 1024), F32),
        ),
        in_specs=[anywhere] * 7,
        out_specs=(inside,) * 4,
        scratch_shapes=[
            pltpu.VMEM((4, 256, 2048), BF),
            pltpu.VMEM((4, 256, 2048), BF),
            pltpu.VMEM((4, 256, 2048), BF),
            pltpu.VMEM((4, 512, 1024), BF),
            pltpu.VMEM((4, 512, 1024), BF),
            pltpu.VMEM((128, 1024), F32),
            pltpu.VMEM((128, 1024), F32),
            pltpu.VMEM((4, 512, 1024), BF),
            pltpu.VMEM((4, 512, 1024), BF),
            pltpu.VMEM((1024, 1024), BF),
            pltpu.VMEM((1024, 1024), BF),
            pltpu.VMEM((1024, 1024), BF),
            pltpu.VMEM((1024, 1024), BF),
            pltpu.VMEM((4, 512, 1024), BF),
            pltpu.VMEM((2, 2, 6, 256, 256), BF),
            pltpu.VMEM((2, 2, 6, 2, 128, 256), BF),
            pltpu.VMEM((2, 2, 2, 6, 64, 256), BF),
            pltpu.VMEM((2, 4, 128, 2048), BF),
            pltpu.VMEM((2, 6, 64, 2048), BF),
            pltpu.SemaphoreType.DMA((7,)),
            pltpu.SemaphoreType.DMA((N_RINGS * 3 + 8,)),
            pltpu.SemaphoreType.DMA((7,)),
        ],
        compiler_params=pltpu.CompilerParams(
            collective_id=0, has_side_effects=True, vmem_limit_bytes=62914560
        ),
        cost_estimate=pl.CostEstimate(
            flops=30064771072, bytes_accessed=32 * 1024 * 1024, transcendentals=0
        ),
    )(
        fresh_rows.reshape(4, 256, 2048), saved_rows.reshape(4, 256, 2048),
        upstream_grad.reshape(4, 256, 2048),
        proj_up, proj_down, accum_up, accum_down,
    )
    return pl.pallas_call(
        settle,
        out_shape=tuple(shape(r.shape, r.dtype) for r in results),
        in_specs=[inside] * 4,
        out_specs=(anywhere,) * 4,
        scratch_shapes=[pltpu.SemaphoreType.DMA((4,))],
    )(*[pltpu.with_memory_space_constraint(r, pltpu.VMEM) for r in results])


def solution(mesh):
    in_specs = (
        P("fs", None),
        P("fs", None),
        P("fs", None),
        P("fs", "tp"),
        P("fs", "tp"),
        P("fs", "tp"),
        P("fs", "tp"),
    )
    out_specs = (P(("fs", "tp"), None), P(("fs", "tp"), None), P("fs", "tp"), P("fs", "tp"))
    return jax.shard_map(body, mesh=mesh, in_specs=in_specs, out_specs=out_specs, check_vma=False)
```

```python
import jax
import jax.numpy as jnp
from jax import lax
from jax.experimental import pallas as pl
from jax.experimental.pallas import tpu as pltpu
from jax.sharding import PartitionSpec as P

MESH = pl.DeviceIdType.MESH
BF = jnp.bfloat16
F32 = jnp.float32
COLS = (slice(0, 512), slice(512, 1024))
GROUPS = tuple((slice(q, q + 256), slice(q + 512, q + 768)) for q in (0, 256))
N_RINGS = 14 + 16 + 2


def rows_at(start, size):
    return pl.ds(pl.multiple_of(start, size), size)


def kernel(
    fresh_hbm, saved_hbm, upstream_hbm, up_hbm, down_hbm, accum_up_hbm, accum_down_hbm,
    fresh_out, saved_grad, accum_up_out, accum_down_out,
    fresh, saved, upstream, up_w, down_w, accum_up, accum_down,
    saved_t, upstream_t, fresh_hidden, saved_active, saved_hidden, pre_grad, grad_down,
    land_z, land_y, land_2, land_pair, land_x,
    send_sem, recv_sem, load_sem,
):
    fs, tp = lax.axis_index("fs"), lax.axis_index("tp")
    z, y, x, core = fs // 4, fs % 4, tp // 2, tp % 2

    def nxt(p, by):
        return lax.rem(p + by, 4)

    to = {
        ("y", 1): (z * 4 + nxt(y, 1), tp),
        ("y", -1): (z * 4 + nxt(y, 3), tp),
        ("z", 1): (nxt(z, 1) * 4 + y, tp),
        ("z", -1): (nxt(z, 3) * 4 + y, tp),
        ("x", 1): (fs, nxt(x, 1) * 2 + core),
        ("x", -1): (fs, nxt(x, 3) * 2 + core),
        "pair": (fs, x * 2 + 1 - core),
    }
    place = {"y": y, "z": z, "x": x}
    used = [0]
    part_of = (slice(None), pl.ds(0, 480))
    bulks = (up_w.at[part_of], down_w.at[part_of], land_z, land_y, land_2, land_x, land_pair)

    def reserve(count):
        used[0] += count
        return used[0] - count

    def message(src, dst, sends, receives, target):
        return pltpu.make_async_remote_copy(
            src_ref=src,
            dst_ref=dst,
            send_sem=send_sem.at[sends],
            recv_sem=recv_sem.at[receives],
            device_id=target,
            device_id_type=MESH,
        )

    class Ring:
        def __init__(self, axis, pool, mate):
            self.plus, self.minus = to[(axis, 1)], to[(axis, -1)]
            p = place[axis]
            self.here, self.after, self.across, self.before = p, nxt(p, 1), nxt(p, 2), nxt(p, 3)
            self.out, self.into = pool, reserve(2)
            self.last = mate.last if mate else reserve(1)

        def push(self, src, dst, slot, target):
            where = self.last if slot == 2 else self.into + slot
            message(src, dst, self.out, where, target).start()

        def got(self, dst, slot):
            where = self.last if slot == 2 else self.into + slot
            message(dst, dst, self.out, where, self.plus).wait_recv()

    class Gather(Ring):
        def __init__(self, axis, block, landed, pool, mate=None):
            super().__init__(axis, pool, mate)
            self.block, self.landed = block, landed

        def go(self, half, slot, owner, target):
            part = self.block(owner, half)
            self.push(part, part, slot, target)

        def start(self):
            self.go(0, 0, self.here, self.plus)
            self.go(1, 1, self.here, self.minus)

        def rest(self):
            self.go(1, 2, self.here, self.plus)
            self.go(0, 2, self.here, self.minus)

        def mid(self):
            self.got(self.block(self.before, 0), 0)
            self.go(0, 2, self.before, self.plus)
            self.got(self.block(self.after, 1), 1)
            self.go(1, 2, self.after, self.minus)

        def end(self):
            if self.landed is not None:
                self.got(self.landed, 2)

    class Scatter(Ring):
        def __init__(self, axis, block, land, landed, pool, mate=None):
            super().__init__(axis, pool, mate)
            self.block, self.land, self.landed = block, land, landed

        def go(self, half, slot, index, owner, target):
            self.push(self.block(owner, half), self.land.at[index], slot, target)

        def add(self, owner, half, index):
            mine = self.block(owner, half)
            mine[...] = (mine[...].astype(F32) + self.land[index].astype(F32)).astype(BF)

        def start(self):
            self.go(0, 0, 0, self.across, self.plus)
            self.go(1, 1, 1, self.across, self.minus)

        def rest(self):
            self.go(1, 2, 2, self.after, self.plus)
            self.go(0, 2, 3, self.before, self.minus)

        def mid(self):
            self.got(self.land.at[0], 0)
            self.add(self.after, 0, 0)
            self.go(0, 2, 4, self.after, self.plus)
            self.got(self.land.at[1], 1)
            self.add(self.before, 1, 1)
            self.go(1, 2, 5, self.before, self.minus)

        def end(self, store):
            if self.landed is not None:
                self.got(self.landed, 2)
            for half, parts in ((0, (3, 4)), (1, (2, 5))):
                total = self.block(self.here, half)[...].astype(F32)
                for index in parts:
                    total = total + self.land[index].astype(F32)
                store(half, total)

    class Both:
        def __init__(self, *rings):
            self.rings = rings

        def __getattr__(self, step):
            def run():
                for ring in self.rings:
                    getattr(ring, step)()
            return run

    def gather_1(w, cols, landed, pool):
        a, b = cols
        one = Gather("y", lambda p, h: w.at[z, rows_at(p * 128 + h * 64, 64), a], landed, pool)
        other = Gather(
            "z", lambda p, h: w.at[p, rows_at(y * 128 + h * 64, 64), b], None, pool, one
        )
        return Both(one, other)

    def gather_2(w, q, pool):
        a, b = GROUPS[q]
        one = Gather("z", lambda p, h: w.at[p, pl.ds(h * 256, 256), a], w.at[0], pool)
        other = Gather(
            "y", lambda p, h: w.at[pl.ds(h * 2, 2), rows_at(p * 128, 128), b], None, pool, one
        )
        return Both(one, other)

    class GradSum:
        def __init__(self, grad, which, q, accum, out):
            a, b = GROUPS[q]
            self.q, self.accum, self.out = q, accum, out
            one = Scatter(
                "z", lambda p, h: grad.at[p, pl.ds(h * 256, 256), a],
                land_z.at[which, q], grad.at[0], 2,
            )
            other = Scatter(
                "y", lambda p, h: grad.at[pl.ds(h * 2, 2), rows_at(p * 128, 128), b],
                land_y.at[which, q], None, 3, one,
            )
            self.one = (one, other)
            one = Scatter(
                "y", lambda p, h: grad.at[z, rows_at(p * 128 + h * 64, 64), a],
                land_2.at[which, q, 0], grad.at[0, pl.ds(0, 128)], 4,
            )
            other = Scatter(
                "z", lambda p, h: grad.at[p, rows_at(y * 128 + h * 64, 64), b],
                land_2.at[which, q, 1], None, 4, one,
            )
            self.two = (one, other)

        def start(self):
            for ring in self.one:
                ring.start()
            for ring in self.one:
                ring.rest()

        def mid(self):
            for ring in self.one:
                ring.mid()

        def turn(self):
            for ring, after in zip(self.one, self.two):
                def keep(half, total, ring=ring):
                    ring.block(ring.here, half)[...] = total.astype(BF)
                ring.end(keep)
                after.start()
                after.rest()

        def mid_2(self):
            for ring in self.two:
                ring.mid()

        def end(self):
            for ring, cols in zip(self.two, GROUPS[self.q]):
                def keep(half, total, cols=cols):
                    rows = pl.ds(half * 64, 64)
                    self.out[rows, cols] = self.accum[rows, cols] + 0.0078125 * total
                ring.end(keep)

    class TokenSum:
        def __init__(self, part, which, out):
            self.part, self.which, self.out = part, which, out
            self.receives = reserve(4)
            self.order = (nxt(x, 2), nxt(x, 1), nxt(x, 3), x)
            self.ring = Scatter(
                "x", lambda p, h: part.at[p, rows_at(core * 128 + h * 64, 64), :],
                land_x.at[which], land_x.at[which, pl.ds(2, 4)], 5,
            )

        def pair(self, src, step):
            return message(
                src, land_pair.at[self.which, step],
                6, self.receives + step, to["pair"],
            )

        def offer(self, *steps):
            for step in steps:
                theirs = self.part.at[self.order[step], rows_at((1 - core) * 128, 128), :]
                self.pair(theirs, step).start()

        def join(self, step):
            landed = land_pair.at[self.which, step]
            self.pair(landed, step).wait_recv()
            mine = self.part.at[self.order[step], rows_at(core * 128, 128), :]
            mine[...] = (mine[...].astype(F32) + landed[...].astype(F32)).astype(BF)

        def end(self):
            def keep(half, total):
                self.out[pl.ds(half * 64, 64), :] = total.astype(BF)
            self.ring.end(keep)

    loads = [
        pltpu.make_async_copy(up_hbm, up_w.at[z, rows_at(y * 128, 128), :], load_sem.at[0]),
        pltpu.make_async_copy(down_hbm, down_w.at[z, rows_at(y * 128, 128), :], load_sem.at[1]),
        pltpu.make_async_copy(saved_hbm, saved, load_sem.at[2]),
        pltpu.make_async_copy(upstream_hbm, upstream, load_sem.at[3]),
        pltpu.make_async_copy(fresh_hbm, fresh, load_sem.at[4]),
        pltpu.make_async_copy(accum_up_hbm, accum_up, load_sem.at[5]),
        pltpu.make_async_copy(accum_down_hbm, accum_down, load_sem.at[6]),
    ]
    for load in loads:
        load.start()

    barrier = pltpu.get_barrier_semaphore()
    for target in to.values():
        pl.semaphore_signal(barrier, inc=1, device_id=target, device_id_type=MESH)
    pl.semaphore_wait(barrier, len(to))

    up_1 = [gather_1(up_w, cols, up_w.at[0, pl.ds(0, 128)], 0) for cols in GROUPS]
    up_2, down_1 = (gather_2(up_w, 0, 0), gather_2(up_w, 1, 0)), gather_1(down_w, COLS, down_w.at[0, pl.ds(0, 256)], 1)
    down_2 = (gather_2(down_w, 0, 1), gather_2(down_w, 1, 1))
    grad_up = upstream_t
    down_sum = [GradSum(grad_down, 0, q, accum_down, accum_down_out) for q in range(2)]
    up_sum = [GradSum(grad_up, 1, q, accum_up, accum_up_out) for q in range(2)]
    fresh_sum = TokenSum(fresh, 0, fresh_out)
    saved_sum = TokenSum(saved, 1, saved_grad)

    def turned(rows, out):
        def step(i, carry):
            out[:, :, rows_at(i * 256, 256)] = rows[i].T.reshape(4, 512, 256)
            return carry
        lax.fori_loop(0, 4, step, 0)

    def hidden(q, rows, weight, store, first=0, last=4):
        def step(j, carry):
            i, ab = j // 2, j % 2
            cols = rows_at(ab * 512 + q * 256, 256)
            pre = jnp.dot(
                rows[pl.ds(i * 2, 2)].reshape(512, 2048),
                weight[:, :, cols].reshape(2048, 256), preferred_element_type=F32,
            )
            store(rows_at(i * 512, 512), cols, pre)
            return carry
        lax.fori_loop(first, last, step, 0)

    def keep_saved(at, cols, pre):
        active = jnp.maximum(pre, 0.0)
        saved_active[at, cols] = active.astype(BF)
        saved_hidden[at, cols] = (active * active).astype(BF)

    def keep_fresh(at, cols, pre):
        active = jnp.maximum(pre, 0.0)
        fresh_hidden[at, cols] = (active * active).astype(BF)

    def keep_back(at, cols, hidden_grad):
        active = saved_active[at, cols].astype(F32)
        pre_grad[at, cols] = (2.0 * active * hidden_grad).astype(BF)

    def grad(q, left, right, out, first=0, last=4):
        a, b = GROUPS[q]
        def step(p, carry):
            total = jnp.dot(left[p], right[:, a], preferred_element_type=F32)
            out[p, :, a] = total.astype(BF)
            total = jnp.dot(left[p], right[:, b], preferred_element_type=F32)
            out[p, :, b] = total.astype(BF)
            return carry
        lax.fori_loop(first, last, step, 0)

    def output(q, hidden_rows, weight, part, chunks, first=0, last=4):
        def beside(block):
            if q is None:
                return block[...]
            a, b = GROUPS[q]
            return jnp.concatenate([block[:, a], block[:, b]], axis=1)
        def step(n, carry):
            left = jnp.concatenate(
                [beside(hidden_rows.at[rows_at(c * 256, 256)]) for c in chunks], axis=0
            )
            total = lax.dot_general(
                left, beside(weight.at[n]), (((1,), (1,)), ((), ())), preferred_element_type=F32
            )
            cols = rows_at(n * 512, 512)
            for k, c in enumerate(chunks):
                some = total[k * 256:k * 256 + 256]
                if q == 1:
                    some = part[c, :, cols].astype(F32) + some
                part[c, :, cols] = some.astype(BF)
            return carry
        lax.fori_loop(first, last, step, 0)

    loads[0].wait()
    loads[1].wait()
    for ring in up_1:
        ring.start()
        ring.rest()
    up_1[0].mid()
    down_1.start()
    down_1.rest()
    up_1[1].mid()
    for load in loads[2:]:
        load.wait()
    up_1[0].end()
    up_2[0].start()
    down_1.mid()
    up_2[0].rest()
    turned(upstream, upstream_t)
    up_2[0].mid()
    up_1[1].end()
    up_2[1].start()
    up_2[1].rest()
    down_1.end()
    turned(saved, saved_t)
    up_2[0].end()

    hidden(0, saved, up_w, keep_saved)
    up_2[1].mid()
    down_2[0].start()
    down_2[0].rest()
    hidden(0, fresh, up_w, keep_fresh)
    grad(0, upstream_t, saved_hidden, grad_down)
    up_2[1].end()
    hidden(1, saved, up_w, keep_saved)
    down_2[0].mid()
    down_2[1].start()
    down_2[1].rest()
    grad(1, upstream_t, saved_hidden, grad_down)
    hidden(1, fresh, up_w, keep_fresh)
    down_2[0].end()
    output(0, fresh_hidden, down_w, fresh, fresh_sum.order[:2])
    down_2[1].mid()
    output(0, fresh_hidden, down_w, fresh, fresh_sum.order[2:])
    pl.when(core == 0)(down_sum[0].start)
    down_2[1].end()

    output(1, fresh_hidden, down_w, fresh, fresh_sum.order[:1])
    fresh_sum.offer(0)
    output(1, fresh_hidden, down_w, fresh, fresh_sum.order[1:2])
    fresh_sum.offer(1)
    pl.when(core == 1)(down_sum[0].start)
    down_sum[1].start()
    output(1, fresh_hidden, down_w, fresh, fresh_sum.order[2:], 0, 2)
    fresh_sum.join(0)
    fresh_sum.ring.start()
    output(1, fresh_hidden, down_w, fresh, fresh_sum.order[2:], 2, 4)
    fresh_sum.offer(2, 3)
    hidden(0, upstream, down_w, keep_back)
    fresh_sum.join(1)
    fresh_sum.join(2)
    fresh_sum.ring.rest()
    fresh_sum.join(3)
    down_sum[0].mid()
    grad(0, saved_t, pre_grad, grad_up)
    up_sum[0].start()
    hidden(1, upstream, down_w, keep_back, 0, 2)
    fresh_sum.ring.mid()
    down_sum[1].mid()
    hidden(1, upstream, down_w, keep_back, 2, 4)
    grad(1, saved_t, pre_grad, grad_up)
    up_sum[1].start()
    output(None, pre_grad, up_w, saved, saved_sum.order[:1])
    saved_sum.offer(0)
    output(None, pre_grad, up_w, saved, saved_sum.order[1:2])
    saved_sum.offer(1)
    saved_sum.join(0)
    saved_sum.ring.start()
    up_sum[0].mid()
    output(None, pre_grad, up_w, saved, saved_sum.order[2:])
    saved_sum.offer(2, 3)
    saved_sum.join(1)
    down_sum[0].turn()
    saved_sum.join(2)
    saved_sum.ring.rest()
    saved_sum.join(3)
    fresh_sum.end()
    up_sum[1].mid()
    down_sum[1].turn()
    saved_sum.ring.mid()
    down_sum[0].mid_2()
    up_sum[0].turn()
    up_sum[1].turn()
    down_sum[1].mid_2()
    up_sum[0].mid_2()
    up_sum[1].mid_2()
    down_sum[0].end()
    down_sum[1].end()
    up_sum[0].end()
    saved_sum.end()
    up_sum[1].end()
    for index, bulk in enumerate(bulks):
        message(bulk, bulk, index, 0, to["pair"]).wait_send()


def settle(*refs):
    held, out, sems = refs[:4], refs[4:8], refs[8]
    copies = [pltpu.make_async_copy(h, o, sems.at[i]) for i, (h, o) in enumerate(zip(held, out))]
    for copy in copies:
        copy.start()
    for copy in copies:
        copy.wait()


def body(fresh_rows, saved_rows, upstream_grad, proj_up, proj_down, accum_up, accum_down):
    anywhere = pl.BlockSpec(memory_space=pl.ANY)
    inside = pl.BlockSpec(memory_space=pltpu.VMEM)
    shape = jax.ShapeDtypeStruct
    results = pl.pallas_call(
        kernel,
        out_shape=(
            pltpu.VMEM((128, 2048), BF), pltpu.VMEM((128, 2048), BF),
            pltpu.VMEM((128, 1024), F32), pltpu.VMEM((128, 1024), F32),
        ),
        in_specs=[anywhere] * 7,
        out_specs=(inside,) * 4,
        scratch_shapes=[
            pltpu.VMEM((4, 256, 2048), BF),
            pltpu.VMEM((4, 256, 2048), BF),
            pltpu.VMEM((4, 256, 2048), BF),
            pltpu.VMEM((4, 512, 1024), BF),
            pltpu.VMEM((4, 512, 1024), BF),
            pltpu.VMEM((128, 1024), F32),
            pltpu.VMEM((128, 1024), F32),
            pltpu.VMEM((4, 512, 1024), BF),
            pltpu.VMEM((4, 512, 1024), BF),
            pltpu.VMEM((1024, 1024), BF),
            pltpu.VMEM((1024, 1024), BF),
            pltpu.VMEM((1024, 1024), BF),
            pltpu.VMEM((1024, 1024), BF),
            pltpu.VMEM((4, 512, 1024), BF),
            pltpu.VMEM((2, 2, 6, 256, 256), BF),
            pltpu.VMEM((2, 2, 6, 2, 128, 256), BF),
            pltpu.VMEM((2, 2, 2, 6, 64, 256), BF),
            pltpu.VMEM((2, 4, 128, 2048), BF),
            pltpu.VMEM((2, 6, 64, 2048), BF),
            pltpu.SemaphoreType.DMA((7,)),
            pltpu.SemaphoreType.DMA((N_RINGS * 3 - 15 + 8,)),
            pltpu.SemaphoreType.DMA((7,)),
        ],
        compiler_params=pltpu.CompilerParams(
            collective_id=0, has_side_effects=True, vmem_limit_bytes=62914560
        ),
        cost_estimate=pl.CostEstimate(
            flops=30064771072, bytes_accessed=32 * 1024 * 1024, transcendentals=0
        ),
    )(
        fresh_rows.reshape(4, 256, 2048), saved_rows.reshape(4, 256, 2048),
        upstream_grad.reshape(4, 256, 2048),
        proj_up, proj_down, accum_up, accum_down,
    )
    return pl.pallas_call(
        settle,
        out_shape=tuple(shape(r.shape, r.dtype) for r in results),
        in_specs=[inside] * 4,
        out_specs=(anywhere,) * 4,
        scratch_shapes=[pltpu.SemaphoreType.DMA((4,))],
    )(*[pltpu.with_memory_space_constraint(r, pltpu.VMEM) for r in results])


def solution(mesh):
    in_specs = (
        P("fs", None),
        P("fs", None),
        P("fs", None),
        P("fs", "tp"),
        P("fs", "tp"),
        P("fs", "tp"),
        P("fs", "tp"),
    )
    out_specs = (P(("fs", "tp"), None), P(("fs", "tp"), None), P("fs", "tp"), P("fs", "tp"))
    return jax.shard_map(body, mesh=mesh, in_specs=in_specs, out_specs=out_specs, check_vma=False)
```

```python
import jax
import jax.numpy as jnp
from jax import lax
from jax.experimental import pallas as pl
from jax.experimental.pallas import tpu as pltpu
from jax.sharding import PartitionSpec as P

MESH = pl.DeviceIdType.MESH
BF = jnp.bfloat16
F32 = jnp.float32
COLS = (slice(0, 512), slice(512, 1024))
GROUPS = tuple((slice(q, q + 256), slice(q + 512, q + 768)) for q in (0, 256))
N_RINGS = 14 + 16 + 2


def rows_at(start, size):
    return pl.ds(pl.multiple_of(start, size), size)


def kernel(
    fresh_hbm, saved_hbm, upstream_hbm, up_hbm, down_hbm, accum_up_hbm, accum_down_hbm,
    fresh_out, saved_grad, accum_up_out, accum_down_out,
    fresh, saved, upstream, up_w, down_w, accum_up, accum_down,
    saved_t, upstream_t, fresh_hidden, saved_active, saved_hidden, pre_grad, grad_down,
    land_z, land_y, land_2, land_pair, land_x,
    send_sem, recv_sem, load_sem,
):
    fs, tp = lax.axis_index("fs"), lax.axis_index("tp")
    z, y, x, core = fs // 4, fs % 4, tp // 2, tp % 2

    def nxt(p, by):
        return lax.rem(p + by, 4)

    to = {
        ("y", 1): (z * 4 + nxt(y, 1), tp),
        ("y", -1): (z * 4 + nxt(y, 3), tp),
        ("z", 1): (nxt(z, 1) * 4 + y, tp),
        ("z", -1): (nxt(z, 3) * 4 + y, tp),
        ("x", 1): (fs, nxt(x, 1) * 2 + core),
        ("x", -1): (fs, nxt(x, 3) * 2 + core),
        "pair": (fs, x * 2 + 1 - core),
    }
    place = {"y": y, "z": z, "x": x}
    used = [0]
    part_of = (slice(None), pl.ds(0, 480))
    bulks = (up_w.at[part_of], down_w.at[part_of], land_z, land_y, land_2, land_x, land_pair)

    def reserve(count):
        used[0] += count
        return used[0] - count

    def message(src, dst, sends, receives, target):
        return pltpu.make_async_remote_copy(
            src_ref=src,
            dst_ref=dst,
            send_sem=send_sem.at[sends],
            recv_sem=recv_sem.at[receives],
            device_id=target,
            device_id_type=MESH,
        )

    class Ring:
        def __init__(self, axis, pool, mate):
            self.plus, self.minus = to[(axis, 1)], to[(axis, -1)]
            p = place[axis]
            self.here, self.after, self.across, self.before = p, nxt(p, 1), nxt(p, 2), nxt(p, 3)
            self.out, self.into = pool, reserve(2)
            self.last = mate.last if mate else reserve(1)

        def push(self, src, dst, slot, target):
            where = self.last if slot == 2 else self.into + slot
            message(src, dst, self.out, where, target).start()

        def got(self, dst, slot):
            where = self.last if slot == 2 else self.into + slot
            message(dst, dst, self.out, where, self.plus).wait_recv()

    class Gather(Ring):
        def __init__(self, axis, block, landed, pool, mate=None):
            super().__init__(axis, pool, mate)
            self.block, self.landed = block, landed

        def go(self, half, slot, owner, target):
            part = self.block(owner, half)
            self.push(part, part, slot, target)

        def start(self):
            self.go(0, 0, self.here, self.plus)
            self.go(1, 1, self.here, self.minus)

        def rest(self):
            self.go(1, 2, self.here, self.plus)
            self.go(0, 2, self.here, self.minus)

        def mid(self):
            self.got(self.block(self.before, 0), 0)
            self.go(0, 2, self.before, self.plus)
            self.got(self.block(self.after, 1), 1)
            self.go(1, 2, self.after, self.minus)

        def end(self):
            if self.landed is not None:
                self.got(self.landed, 2)

    class Scatter(Ring):
        def __init__(self, axis, block, land, landed, pool, mate=None):
            super().__init__(axis, pool, mate)
            self.block, self.land, self.landed = block, land, landed

        def go(self, half, slot, index, owner, target):
            self.push(self.block(owner, half), self.land.at[index], slot, target)

        def add(self, owner, half, index):
            mine = self.block(owner, half)
            mine[...] = (mine[...].astype(F32) + self.land[index].astype(F32)).astype(BF)

        def start(self):
            self.go(0, 0, 0, self.across, self.plus)
            self.go(1, 1, 1, self.across, self.minus)

        def rest(self):
            self.go(1, 2, 2, self.after, self.plus)
            self.go(0, 2, 3, self.before, self.minus)

        def mid(self):
            self.got(self.land.at[0], 0)
            self.add(self.after, 0, 0)
            self.go(0, 2, 4, self.after, self.plus)
            self.got(self.land.at[1], 1)
            self.add(self.before, 1, 1)
            self.go(1, 2, 5, self.before, self.minus)

        def end(self, store):
            if self.landed is not None:
                self.got(self.landed, 2)
            for half, parts in ((0, (3, 4)), (1, (2, 5))):
                total = self.block(self.here, half)[...].astype(F32)
                for index in parts:
                    total = total + self.land[index].astype(F32)
                store(half, total)

    class Both:
        def __init__(self, *rings):
            self.rings = rings

        def __getattr__(self, step):
            def run():
                for ring in self.rings:
                    getattr(ring, step)()
            return run

    def gather_1(w, cols, landed, pool):
        a, b = cols
        one = Gather("y", lambda p, h: w.at[z, rows_at(p * 128 + h * 64, 64), a], landed, pool)
        other = Gather(
            "z", lambda p, h: w.at[p, rows_at(y * 128 + h * 64, 64), b], None, pool, one
        )
        return Both(one, other)

    def gather_2(w, q, pool):
        a, b = GROUPS[q]
        one = Gather("z", lambda p, h: w.at[p, pl.ds(h * 256, 256), a], w.at[0], pool)
        other = Gather(
            "y", lambda p, h: w.at[pl.ds(h * 2, 2), rows_at(p * 128, 128), b], None, pool, one
        )
        return Both(one, other)

    class GradSum:
        def __init__(self, grad, which, q, accum, out):
            a, b = GROUPS[q]
            self.q, self.accum, self.out = q, accum, out
            one = Scatter(
                "z", lambda p, h: grad.at[p, pl.ds(h * 256, 256), a],
                land_z.at[which, q], grad.at[0], 2,
            )
            other = Scatter(
                "y", lambda p, h: grad.at[pl.ds(h * 2, 2), rows_at(p * 128, 128), b],
                land_y.at[which, q], None, 3, one,
            )
            self.one = (one, other)
            one = Scatter(
                "y", lambda p, h: grad.at[z, rows_at(p * 128 + h * 64, 64), a],
                land_2.at[which, q, 0], grad.at[0, pl.ds(0, 128)], 4,
            )
            other = Scatter(
                "z", lambda p, h: grad.at[p, rows_at(y * 128 + h * 64, 64), b],
                land_2.at[which, q, 1], None, 4, one,
            )
            self.two = (one, other)

        def start(self):
            for ring in self.one:
                ring.start()
            for ring in self.one:
                ring.rest()

        def mid(self):
            for ring in self.one:
                ring.mid()

        def turn(self):
            for ring, after in zip(self.one, self.two):
                def keep(half, total, ring=ring):
                    ring.block(ring.here, half)[...] = total.astype(BF)
                ring.end(keep)
                after.start()
                after.rest()

        def mid_2(self):
            for ring in self.two:
                ring.mid()

        def end(self):
            for ring, cols in zip(self.two, GROUPS[self.q]):
                def keep(half, total, cols=cols):
                    rows = pl.ds(half * 64, 64)
                    self.out[rows, cols] = self.accum[rows, cols] + 0.0078125 * total
                ring.end(keep)

    class TokenSum:
        def __init__(self, part, which, out):
            self.part, self.which, self.out = part, which, out
            self.receives = reserve(4)
            self.order = (nxt(x, 2), nxt(x, 1), nxt(x, 3), x)
            self.ring = Scatter(
                "x", lambda p, h: part.at[p, rows_at(core * 128 + h * 64, 64), :],
                land_x.at[which], land_x.at[which, pl.ds(2, 4)], 5,
            )

        def pair(self, src, step):
            return message(
                src, land_pair.at[self.which, step],
                6, self.receives + step, to["pair"],
            )

        def offer(self, *steps):
            for step in steps:
                theirs = self.part.at[self.order[step], rows_at((1 - core) * 128, 128), :]
                self.pair(theirs, step).start()

        def join(self, step):
            landed = land_pair.at[self.which, step]
            self.pair(landed, step).wait_recv()
            mine = self.part.at[self.order[step], rows_at(core * 128, 128), :]
            mine[...] = (mine[...].astype(F32) + landed[...].astype(F32)).astype(BF)

        def end(self):
            def keep(half, total):
                self.out[pl.ds(half * 64, 64), :] = total.astype(BF)
            self.ring.end(keep)

    loads = [
        pltpu.make_async_copy(up_hbm, up_w.at[z, rows_at(y * 128, 128), :], load_sem.at[0]),
        pltpu.make_async_copy(down_hbm, down_w.at[z, rows_at(y * 128, 128), :], load_sem.at[1]),
        pltpu.make_async_copy(saved_hbm, saved, load_sem.at[2]),
        pltpu.make_async_copy(upstream_hbm, upstream, load_sem.at[3]),
        pltpu.make_async_copy(fresh_hbm, fresh, load_sem.at[4]),
        pltpu.make_async_copy(accum_up_hbm, accum_up, load_sem.at[5]),
        pltpu.make_async_copy(accum_down_hbm, accum_down, load_sem.at[6]),
    ]
    for load in loads:
        load.start()

    barrier = pltpu.get_barrier_semaphore()
    for target in to.values():
        pl.semaphore_signal(barrier, inc=1, device_id=target, device_id_type=MESH)
    pl.semaphore_wait(barrier, len(to))

    up_1 = [gather_1(up_w, cols, up_w.at[0, pl.ds(0, 128)], 0) for cols in GROUPS]
    up_2, down_1 = (gather_2(up_w, 0, 0), gather_2(up_w, 1, 0)), gather_1(down_w, COLS, down_w.at[0, pl.ds(0, 256)], 1)
    down_2 = (gather_2(down_w, 0, 1), gather_2(down_w, 1, 1))
    grad_up = upstream_t
    down_sum = [GradSum(grad_down, 0, q, accum_down, accum_down_out) for q in range(2)]
    up_sum = [GradSum(grad_up, 1, q, accum_up, accum_up_out) for q in range(2)]
    fresh_sum = TokenSum(fresh, 0, fresh_out)
    saved_sum = TokenSum(saved, 1, saved_grad)

    def turned(rows, out):
        def step(i, carry):
            out[:, :, rows_at(i * 256, 256)] = rows[i].T.reshape(4, 512, 256)
            return carry
        lax.fori_loop(0, 4, step, 0)

    def hidden(q, rows, weight, store, first=0, last=4):
        def step(j, carry):
            i, ab = j // 2, j % 2
            cols = rows_at(ab * 512 + q * 256, 256)
            pre = jnp.dot(
                rows[pl.ds(i * 2, 2)].reshape(512, 2048),
                weight[:, :, cols].reshape(2048, 256), preferred_element_type=F32,
            )
            store(rows_at(i * 512, 512), cols, pre)
            return carry
        lax.fori_loop(first, last, step, 0)

    def keep_saved(at, cols, pre):
        active = jnp.maximum(pre, 0.0)
        saved_active[at, cols] = active.astype(BF)
        saved_hidden[at, cols] = (active * active).astype(BF)

    def keep_fresh(at, cols, pre):
        active = jnp.maximum(pre, 0.0)
        fresh_hidden[at, cols] = (active * active).astype(BF)

    def keep_back(at, cols, hidden_grad):
        active = saved_active[at, cols].astype(F32)
        pre_grad[at, cols] = (2.0 * active * hidden_grad).astype(BF)

    def grad(q, left, right, out, first=0, last=4):
        a, b = GROUPS[q]
        def step(p, carry):
            total = jnp.dot(left[p], right[:, a], preferred_element_type=F32)
            out[p, :, a] = total.astype(BF)
            total = jnp.dot(left[p], right[:, b], preferred_element_type=F32)
            out[p, :, b] = total.astype(BF)
            return carry
        lax.fori_loop(first, last, step, 0)

    def output(q, hidden_rows, weight, part, chunks, first=0, last=4):
        def beside(block):
            if q is None:
                return block[...]
            a, b = GROUPS[q]
            return jnp.concatenate([block[:, a], block[:, b]], axis=1)
        def step(n, carry):
            left = jnp.concatenate(
                [beside(hidden_rows.at[rows_at(c * 256, 256)]) for c in chunks], axis=0
            )
            total = lax.dot_general(
                left, beside(weight.at[n]), (((1,), (1,)), ((), ())), preferred_element_type=F32
            )
            cols = rows_at(n * 512, 512)
            for k, c in enumerate(chunks):
                some = total[k * 256:k * 256 + 256]
                if q == 1:
                    some = part[c, :, cols].astype(F32) + some
                part[c, :, cols] = some.astype(BF)
            return carry
        lax.fori_loop(first, last, step, 0)

    loads[0].wait()
    loads[1].wait()
    for ring in up_1:
        ring.start()
        ring.rest()
    up_1[0].mid()
    down_1.start()
    down_1.rest()
    up_1[1].mid()
    for load in loads[2:]:
        load.wait()
    up_1[0].end()
    up_2[0].start()
    down_1.mid()
    up_2[0].rest()
    turned(upstream, upstream_t)
    up_2[0].mid()
    up_1[1].end()
    up_2[1].start()
    up_2[1].rest()
    down_1.end()
    turned(saved, saved_t)
    up_2[0].end()

    hidden(0, saved, up_w, keep_saved)
    up_2[1].mid()
    down_2[0].start()
    down_2[0].rest()
    hidden(0, fresh, up_w, keep_fresh)
    grad(0, upstream_t, saved_hidden, grad_down)
    up_2[1].end()
    hidden(1, saved, up_w, keep_saved)
    down_2[0].mid()
    down_2[1].start()
    down_2[1].rest()
    grad(1, upstream_t, saved_hidden, grad_down)
    hidden(1, fresh, up_w, keep_fresh)
    down_2[0].end()
    output(0, fresh_hidden, down_w, fresh, fresh_sum.order[:2])
    down_2[1].mid()
    output(0, fresh_hidden, down_w, fresh, fresh_sum.order[2:])
    pl.when(core == 0)(down_sum[0].start)
    down_2[1].end()
    pl.when(core == 0)(down_sum[1].start)

    output(1, fresh_hidden, down_w, fresh, fresh_sum.order[:1])
    fresh_sum.offer(0)
    output(1, fresh_hidden, down_w, fresh, fresh_sum.order[1:2])
    fresh_sum.offer(1)
    pl.when(core == 1)(down_sum[0].start)
    pl.when(core == 1)(down_sum[1].start)
    output(1, fresh_hidden, down_w, fresh, fresh_sum.order[2:], 0, 2)
    fresh_sum.join(0)
    fresh_sum.ring.start()
    output(1, fresh_hidden, down_w, fresh, fresh_sum.order[2:], 2, 4)
    fresh_sum.offer(2, 3)
    hidden(0, upstream, down_w, keep_back)
    fresh_sum.join(1)
    fresh_sum.join(2)
    fresh_sum.ring.rest()
    fresh_sum.join(3)
    down_sum[0].mid()
    grad(0, saved_t, pre_grad, grad_up)
    up_sum[0].start()
    hidden(1, upstream, down_w, keep_back, 0, 2)
    fresh_sum.ring.mid()
    down_sum[1].mid()
    hidden(1, upstream, down_w, keep_back, 2, 4)
    grad(1, saved_t, pre_grad, grad_up)
    up_sum[1].start()
    output(None, pre_grad, up_w, saved, saved_sum.order[:1])
    saved_sum.offer(0)
    output(None, pre_grad, up_w, saved, saved_sum.order[1:2])
    saved_sum.offer(1)
    saved_sum.join(0)
    saved_sum.ring.start()
    up_sum[0].mid()
    output(None, pre_grad, up_w, saved, saved_sum.order[2:])
    saved_sum.offer(2, 3)
    saved_sum.join(1)
    down_sum[0].turn()
    saved_sum.join(2)
    saved_sum.ring.rest()
    saved_sum.join(3)
    fresh_sum.end()
    up_sum[1].mid()
    down_sum[1].turn()
    saved_sum.ring.mid()
    down_sum[0].mid_2()
    up_sum[0].turn()
    up_sum[1].turn()
    down_sum[1].mid_2()
    up_sum[0].mid_2()
    up_sum[1].mid_2()
    down_sum[0].end()
    down_sum[1].end()
    up_sum[0].end()
    saved_sum.end()
    up_sum[1].end()
    for index, bulk in enumerate(bulks):
        message(bulk, bulk, index, 0, to["pair"]).wait_send()


def settle(*refs):
    held, out, sems = refs[:4], refs[4:8], refs[8]
    copies = [pltpu.make_async_copy(h, o, sems.at[i]) for i, (h, o) in enumerate(zip(held, out))]
    for copy in copies:
        copy.start()
    for copy in copies:
        copy.wait()


def body(fresh_rows, saved_rows, upstream_grad, proj_up, proj_down, accum_up, accum_down):
    anywhere = pl.BlockSpec(memory_space=pl.ANY)
    inside = pl.BlockSpec(memory_space=pltpu.VMEM)
    shape = jax.ShapeDtypeStruct
    results = pl.pallas_call(
        kernel,
        out_shape=(
            pltpu.VMEM((128, 2048), BF), pltpu.VMEM((128, 2048), BF),
            pltpu.VMEM((128, 1024), F32), pltpu.VMEM((128, 1024), F32),
        ),
        in_specs=[anywhere] * 7,
        out_specs=(inside,) * 4,
        scratch_shapes=[
            pltpu.VMEM((4, 256, 2048), BF),
            pltpu.VMEM((4, 256, 2048), BF),
            pltpu.VMEM((4, 256, 2048), BF),
            pltpu.VMEM((4, 512, 1024), BF),
            pltpu.VMEM((4, 512, 1024), BF),
            pltpu.VMEM((128, 1024), F32),
            pltpu.VMEM((128, 1024), F32),
            pltpu.VMEM((4, 512, 1024), BF),
            pltpu.VMEM((4, 512, 1024), BF),
            pltpu.VMEM((1024, 1024), BF),
            pltpu.VMEM((1024, 1024), BF),
            pltpu.VMEM((1024, 1024), BF),
            pltpu.VMEM((1024, 1024), BF),
            pltpu.VMEM((4, 512, 1024), BF),
            pltpu.VMEM((2, 2, 6, 256, 256), BF),
            pltpu.VMEM((2, 2, 6, 2, 128, 256), BF),
            pltpu.VMEM((2, 2, 2, 6, 64, 256), BF),
            pltpu.VMEM((2, 4, 128, 2048), BF),
            pltpu.VMEM((2, 6, 64, 2048), BF),
            pltpu.SemaphoreType.DMA((7,)),
            pltpu.SemaphoreType.DMA((N_RINGS * 3 - 15 + 8,)),
            pltpu.SemaphoreType.DMA((7,)),
        ],
        compiler_params=pltpu.CompilerParams(
            collective_id=0, has_side_effects=True, vmem_limit_bytes=62914560
        ),
        cost_estimate=pl.CostEstimate(
            flops=30064771072, bytes_accessed=32 * 1024 * 1024, transcendentals=0
        ),
    )(
        fresh_rows.reshape(4, 256, 2048), saved_rows.reshape(4, 256, 2048),
        upstream_grad.reshape(4, 256, 2048),
        proj_up, proj_down, accum_up, accum_down,
    )
    return pl.pallas_call(
        settle,
        out_shape=tuple(shape(r.shape, r.dtype) for r in results),
        in_specs=[inside] * 4,
        out_specs=(anywhere,) * 4,
        scratch_shapes=[pltpu.SemaphoreType.DMA((4,))],
    )(*[pltpu.with_memory_space_constraint(r, pltpu.VMEM) for r in results])


def solution(mesh):
    in_specs = (
        P("fs", None),
        P("fs", None),
        P("fs", None),
        P("fs", "tp"),
        P("fs", "tp"),
        P("fs", "tp"),
        P("fs", "tp"),
    )
    out_specs = (P(("fs", "tp"), None), P(("fs", "tp"), None), P("fs", "tp"), P("fs", "tp"))
    return jax.shard_map(body, mesh=mesh, in_specs=in_specs, out_specs=out_specs, check_vma=False)
```
